256 devices in a mesh: dp: 4 (over x), kv: 32 (over z, y), tp: 2 (over core).
Axes of the slice: x: 4, y: 4, z: 8, core: 2. Of those that a mesh axis runs over, the one named last changes fastest.
Arguments:
- tokens: bfloat16 [4, 16384, 1024], P('dp', ('kv', 'tp')), may hold values from -6 to 6
- w_query: bfloat16 [1024, 1024], P(None, 'tp'), may hold values from -0.1875 to 0.1875
- w_key: bfloat16 [1024, 256], P(None, 'tp'), may hold values from -0.1875 to 0.1875
- w_value: bfloat16 [1024, 256], P(None, 'tp'), may hold values from -0.1875 to 0.1875
- w_out: bfloat16 [1024, 1024], P('tp'), may hold values from -0.1875 to 0.1875
- chosen: int32 [4, 256, 15], P('dp', 'kv'), may hold values from -1 to 254, as said below
Outputs:
- normed: bfloat16 [4, 16384, 1024], P('dp', ('kv', 'tp'))
- logsums: float32 [4, 16384, 16], P('dp', 'kv', 'tp')
The draws below stay inside these ranges and needn't reach their ends.
Inputs may be any that keep to these rules, and one draw needn't show every extreme that they name: Each entry of chosen[s, c] is -1 or a block below c; entries of a row that are not -1 differ. Within a sequence, the 15 times 8 entries of the query blocks of one aligned run of 8 blocks name at most 4 different blocks inside any one aligned run, and some run pair reaches exactly 4.
All inputs are finite; a program needn't handle non-finite values.
Results may differ from the reference program's by a relative error of at most 0.0085.
Values may be sent and summed in bfloat16 or wider, within the bound.
No kernel may reach another device: no remote copies, remote signals or barrier semaphores. Data moves between devices by JAX's collectives and lax.ppermute only.
A program may use at most 64 MiB of HBM per device.

```python
import jax
import jax.numpy as jnp
from jax import lax

D = 1024
HEADS = 16
KV_HEADS = 4
HEAD_DIM = 64
BLK = 64
PICK = 15
CAP = 4
TOK_DEV = 512
SEQS = 4
SEQ = 16384
NBLK = 256


def draw_chosen(key, part):
    local_blocks = TOK_DEV // BLK
    owner_count = NBLK // local_blocks
    key_pool = jax.random.fold_in(key, 11)
    key_popular = jax.random.fold_in(key, 23)
    key_noise = jax.random.fold_in(key, 37)
    pool_scores = jax.random.randint(key_pool, (SEQS, owner_count, owner_count, local_blocks), 0, 4096) * local_blocks
    pool_scores = pool_scores + jnp.arange(local_blocks, dtype=jnp.int32)
    ranking = jnp.argsort(jnp.argsort(pool_scores, axis=-1, stable=True), axis=-1, stable=True)
    member = (ranking < CAP).reshape(SEQS, owner_count, NBLK)
    blocks = jnp.arange(NBLK, dtype=jnp.int32)
    owners = blocks // local_blocks
    earlier_owner = owners[None, :] <= jnp.arange(owner_count, dtype=jnp.int32)[:, None]
    member = member & earlier_owner[None]
    candidate = member[:, owners, :] & (blocks[None, :] < blocks[:, None])[None]
    last_block = blocks % local_blocks == local_blocks - 1
    forced = last_block[:, None] & (owners[None, :] == owners[:, None] - 1)
    popularity = jax.random.randint(key_popular, (SEQS, owner_count), 0, 8)
    noise = jax.random.randint(key_noise, (SEQS, NBLK, NBLK), 0, 2048)
    score = candidate.astype(jnp.int32) * 2 ** 27
    score = score + (forced[None] & candidate).astype(jnp.int32) * 2 ** 26
    score = score + popularity[:, None, :][:, :, owners] * 2 ** 22
    score = score + noise * NBLK + blocks[None, None, :]
    ordered, picked = lax.top_k(score, PICK)
    taken = jnp.take_along_axis(candidate, picked, axis=-1)
    return jnp.where(taken, picked, -1).astype(jnp.int32)


def level_of(own_key, extent, pieces, low, largest):
    gain = 1.0
    for position, parts in pieces:
        steps = jax.random.uniform(jax.random.fold_in(jax.random.fold_in(own_key, 6), position), (parts,), jnp.float32, low / len(pieces), largest / len(pieces))
        gain = gain * jnp.repeat(jnp.exp(steps), extent[position] // parts).reshape((-1,) + (1,) * (len(extent) - 1 - position))
    return gain


def normal_values(key, shape, width, reach, pieces=(), held_as=jnp.bfloat16):
    drawn = jax.random.normal(key, shape, jnp.float32) * width
    if len(pieces) > 0:
        drawn = level_of(key, shape, pieces, -0.22, 0.18) * drawn
    return jnp.clip(drawn, min=-reach, max=reach).astype(held_as)


def setup_inputs(seed: int = 0) -> dict:
    seeds = jax.random.split(jax.random.key(seed), 7)
    tokens = normal_values(seeds[0], (SEQS, SEQ, D), 1.0, 6.0, ((0, 4), (1, 64)))
    w_query = normal_values(seeds[1], (D, HEADS * HEAD_DIM), D ** -0.5, 0.1875, ((1, 2),))
    w_key = normal_values(seeds[2], (D, KV_HEADS * HEAD_DIM), D ** -0.5, 0.1875, ((1, 2),))
    w_value = normal_values(seeds[3], (D, KV_HEADS * HEAD_DIM), D ** -0.5, 0.1875, ((1, 2),))
    w_out = normal_values(seeds[4], (HEADS * HEAD_DIM, D), (HEADS * HEAD_DIM) ** -0.5, 0.1875, ((0, 2),))
    chosen = draw_chosen(jax.random.fold_in(seeds[6], 71), 0)
    return {"tokens": tokens, "w_query": w_query, "w_key": w_key, "w_value": w_value, "w_out": w_out, "chosen": chosen}


THETA_BASE = 10000.0
NEGATIVE = -1e+30
EPSILON = 1e-06

def rotate(values_in, positions):
    half_width = values_in.shape[-1] // 2
    inverse = THETA_BASE ** (-jnp.arange(half_width, dtype=jnp.float32) / half_width)
    angles = positions.astype(jnp.float32)[:, None] * inverse[None, :]
    cosine_table = jnp.cos(angles)[:, None, :]
    sine_table = jnp.sin(angles)[:, None, :]
    as_float = values_in.astype(jnp.float32)
    first_half = as_float[..., :half_width]
    second_half = as_float[..., half_width:]
    joined = jnp.concatenate([first_half * cosine_table - second_half * sine_table, second_half * cosine_table + first_half * sine_table], axis=-1)
    return joined.astype(jnp.bfloat16)

def attend(queries, key_rows, value_rows, usable):
    scores = jnp.einsum('qkgd,nkd->kgqn', queries.astype(jnp.float32), key_rows.astype(jnp.float32))
    scores = scores * HEAD_DIM ** (-0.5)
    scores = jnp.where(usable[None, None], scores, NEGATIVE)
    maximum = lax.optimization_barrier(jnp.max(scores, axis=-1, keepdims=True))
    exponent = jnp.exp(scores - maximum)
    denominator = lax.optimization_barrier(jnp.sum(exponent, axis=-1, keepdims=True))
    logsum = (maximum + jnp.log(denominator))[..., 0]
    weights = (exponent / denominator).astype(jnp.bfloat16)
    combined = jnp.einsum('kgqn,nkd->qkgd', weights.astype(jnp.float32), value_rows.astype(jnp.float32))
    block_rows = queries.shape[0]
    return (combined.astype(jnp.bfloat16).reshape(block_rows, -1), jnp.transpose(logsum, (2, 0, 1)).reshape(block_rows, -1))

def block_mask(usable_picks):
    picked_keys = jnp.repeat(usable_picks, BLK)
    earlier = jnp.broadcast_to(picked_keys[None, :], (BLK, PICK * BLK))
    query_pos = jnp.arange(BLK, dtype=jnp.int32)
    causal = query_pos[None, :] <= query_pos[:, None]
    return jnp.concatenate([earlier, causal], axis=1)

def reference(tokens, w_query, w_key, w_value, w_out, chosen):
    group_size = HEADS // KV_HEADS
    positions = jnp.arange(SEQ, dtype=jnp.int32)

    def one_sequence(element):
        rows_in, chosen_rows = element
        queries = jnp.dot(rows_in, w_query, preferred_element_type=jnp.float32).astype(jnp.bfloat16)
        key_rows = jnp.dot(rows_in, w_key, preferred_element_type=jnp.float32).astype(jnp.bfloat16)
        value_rows = jnp.dot(rows_in, w_value, preferred_element_type=jnp.float32).astype(jnp.bfloat16)
        queries = rotate(queries.reshape(SEQ, HEADS, HEAD_DIM), positions)
        key_rows = rotate(key_rows.reshape(SEQ, KV_HEADS, HEAD_DIM), positions)
        value_rows = value_rows.reshape(SEQ, KV_HEADS, HEAD_DIM)
        query_blocks = queries.reshape(NBLK, BLK, KV_HEADS, group_size, HEAD_DIM)
        key_blocks = key_rows.reshape(NBLK, BLK, KV_HEADS, HEAD_DIM)
        value_blocks = value_rows.reshape(NBLK, BLK, KV_HEADS, HEAD_DIM)

        def one_block(item):
            block_index, block_picks = item
            usable_picks = block_picks >= 0
            safe_index = jnp.maximum(block_picks, 0).astype(jnp.int32)
            gathered_keys = jnp.concatenate([key_blocks[safe_index].reshape(PICK * BLK, KV_HEADS, HEAD_DIM), key_blocks[block_index]], axis=0)
            gathered_values = jnp.concatenate([value_blocks[safe_index].reshape(PICK * BLK, KV_HEADS, HEAD_DIM), value_blocks[block_index]], axis=0)
            return attend(query_blocks[block_index], gathered_keys, gathered_values, block_mask(usable_picks))
        outputs, block_logs = lax.map(one_block, (jnp.arange(NBLK, dtype=jnp.int32), chosen_rows))
        attended = outputs.reshape(SEQ, HEADS * HEAD_DIM)
        projected = jnp.dot(attended, w_out, preferred_element_type=jnp.float32)
        scale_rows = lax.rsqrt(lax.optimization_barrier(jnp.mean(projected * projected, axis=-1, keepdims=True)) + EPSILON)
        return ((projected * scale_rows).astype(jnp.bfloat16), block_logs.reshape(SEQ, HEADS))
    normed, logsums = lax.map(one_sequence, (tokens, chosen))
    return (normed, logsums)
```

```python
import functools

import jax
import jax.numpy as jnp
from jax import lax
from jax.experimental import pallas as pl
from jax.experimental.pallas import tpu as pltpu
from jax.sharding import PartitionSpec as P

HEAD_DIM = 64
BLK = 64
PICK = 15
THETA_BASE = 10000.0
NEGATIVE = -1e30
EPSILON = 1e-06
LANES = 128


def rotary_tables(positions):
    half = HEAD_DIM // 2
    inverse = THETA_BASE ** (-jnp.arange(half, dtype=jnp.float32) / half)
    angles = positions.astype(jnp.float32)[:, None] * inverse[None, :]
    cosine = jnp.cos(angles)
    sine = jnp.sin(angles)
    return (
        jnp.concatenate([cosine] * 4, axis=1),
        jnp.concatenate([-sine, sine, -sine, sine], axis=1),
    )


def rotated(values, cosine, sine):
    lane = lax.broadcasted_iota(jnp.int32, values.shape, 1)
    ahead = pltpu.roll(values, LANES - HEAD_DIM // 2, 1)
    behind = pltpu.roll(values, HEAD_DIM // 2, 1)
    swapped = jnp.where(lane % HEAD_DIM < HEAD_DIM // 2, ahead, behind)
    return values * cosine + swapped * sine


def rounded(x):
    return x.astype(jnp.bfloat16).astype(jnp.float32)


def kv_kernel(own_ref, peer_ref, wk_ref, wv_ref, cos_ref, sin_ref, out_ref):
    half = own_ref.shape[0]
    for side, src in enumerate((own_ref, peer_ref)):
        rows = pl.ds(side * half, half)
        piece = src[...]
        keys = rounded(jnp.dot(piece, wk_ref[...], preferred_element_type=jnp.float32))
        out_ref[rows, :LANES] = rotated(keys, cos_ref[rows, :], sin_ref[rows, :]).astype(
            jnp.bfloat16
        )
        out_ref[rows, LANES:] = jnp.dot(
            piece, wv_ref[...], preferred_element_type=jnp.float32
        ).astype(jnp.bfloat16)


def q_kernel(own_ref, peer_ref, wq_ref, cos_ref, sin_ref, out_ref):
    half = own_ref.shape[0]
    for side, src in enumerate((own_ref, peer_ref)):
        rows = pl.ds(side * half, half)
        whole = rounded(jnp.dot(src[...], wq_ref[...], preferred_element_type=jnp.float32))
        for g in range(whole.shape[1] // LANES):
            cols = slice(g * LANES, (g + 1) * LANES)
            turned = rotated(whole[:, cols], cos_ref[rows, :], sin_ref[rows, :])
            out_ref[rows, cols] = turned.astype(jnp.bfloat16) * jnp.bfloat16(HEAD_DIM**-0.5)


def attend_kernel(
    group, slots_ref, usable_ref, q_ref, kv_ref, att_ref, lse_ref, held, bias, sems
):
    step = pl.program_id(0)
    count = pl.num_programs(0)
    keys_wide = (PICK + 1) * BLK

    def fetch(which, slot):
        for p in range(PICK + 1):
            pltpu.make_async_copy(
                kv_ref.at[slots_ref[which, p]], held.at[slot, pl.ds(p * BLK, BLK)], sems.at[slot]
            ).start()

    @pl.when(step == 0)
    def _():
        fetch(0, 0)

    slot = lax.rem(step, 2)

    @pl.when(step + 1 < count)
    def _():
        fetch(step + 1, 1 - slot)

    lane = lax.broadcasted_iota(jnp.int32, (1, LANES), 1)
    for pair in range(keys_wide // LANES):
        left = usable_ref[step, 2 * pair]
        right = usable_ref[step, 2 * pair + 1]
        flag = jnp.where(lane < BLK, left, right)
        bias[:, pair * LANES : (pair + 1) * LANES] = jnp.where(flag > 0, 0.0, NEGATIVE)

    pltpu.make_async_copy(held.at[slot], held.at[slot], sems.at[slot]).wait()

    half_lane = lax.broadcasted_iota(jnp.int32, (BLK, LANES), 1) < HEAD_DIM
    row = lax.broadcasted_iota(jnp.int32, (BLK, LANES), 0)
    col = lax.broadcasted_iota(jnp.int32, (BLK, LANES), 1)
    causal = (col < BLK) | (col - BLK <= row)
    causal = jnp.concatenate([causal] * group, axis=0)
    keys = held[slot, :, :LANES]
    values = held[slot, :, LANES:]
    results = []
    logs = []
    for k in range(2):
        pieces = []
        for g in range(group):
            tile = q_ref[:, g * LANES : (g + 1) * LANES]
            keep = half_lane if k == 0 else ~half_lane
            pieces.append(jnp.where(keep, tile, jnp.zeros_like(tile)))
        stacked = jnp.concatenate(pieces, axis=0)
        scores = lax.dot_general(
            stacked, keys, (((1,), (1,)), ((), ())), preferred_element_type=jnp.float32
        )
        scores = scores + bias[...]
        tail = jnp.where(causal, scores[:, keys_wide - LANES :], NEGATIVE)
        scores = jnp.concatenate([scores[:, : keys_wide - LANES], tail], axis=1)
        top = jnp.max(scores, axis=1, keepdims=True)
        exponent = jnp.exp(scores - top)
        total = jnp.sum(exponent, axis=1, keepdims=True)
        mixed = jnp.dot(
            exponent.astype(jnp.bfloat16), values, preferred_element_type=jnp.float32
        )
        results.append(mixed / total)
        logs.append(top + jnp.log(total))
    for g in range(group):
        rows = slice(g * BLK, (g + 1) * BLK)
        att_ref[:, g * LANES : (g + 1) * LANES] = jnp.where(
            half_lane, results[0][rows], results[1][rows]
        ).astype(jnp.bfloat16)
    wide = lax.broadcasted_iota(jnp.int32, (BLK, 2 * group), 1)
    lse = jnp.zeros((BLK, 2 * group), jnp.float32)
    for k in range(2):
        for g in range(group):
            lse = jnp.where(wide == k * group + g, logs[k][g * BLK : (g + 1) * BLK], lse)
    lse_ref[...] = lse


def finish_kernel(part_ref, peer_ref, w_ref, out_ref):
    projected = part_ref[...] + jnp.dot(
        peer_ref[...], w_ref[...], preferred_element_type=jnp.float32
    )
    scale = lax.rsqrt(jnp.mean(projected * projected, axis=1, keepdims=True) + EPSILON)
    out_ref[...] = (projected * scale).astype(jnp.bfloat16)


def attend(q_rows, kv_all, slots, usable):
    rows, width = q_rows.shape
    steps = rows // BLK
    group = width // LANES
    grid_spec = pltpu.PrefetchScalarGridSpec(
        num_scalar_prefetch=2,
        grid=(steps,),
        in_specs=[
            pl.BlockSpec((BLK, width), lambda i, *_: (i, 0)),
            pl.BlockSpec(memory_space=pl.ANY),
        ],
        out_specs=[
            pl.BlockSpec((BLK, width), lambda i, *_: (i, 0)),
            pl.BlockSpec((BLK, 2 * group), lambda i, *_: (i, 0)),
        ],
        scratch_shapes=[
            pltpu.VMEM((2, (PICK + 1) * BLK, 2 * LANES), jnp.bfloat16),
            pltpu.VMEM((1, (PICK + 1) * BLK), jnp.float32),
            pltpu.SemaphoreType.DMA((2,)),
        ],
    )
    return pl.pallas_call(
        functools.partial(attend_kernel, group),
        grid_spec=grid_spec,
        out_shape=[
            jax.ShapeDtypeStruct((rows, width), jnp.bfloat16),
            jax.ShapeDtypeStruct((rows, 2 * group), jnp.float32),
        ],
        cost_estimate=pl.CostEstimate(
            flops=4 * rows * width * (PICK + 1) * BLK,
            bytes_accessed=steps * (PICK + 1) * BLK * 512,
            transcendentals=0,
        ),
        name="attend",
    )(slots, usable, q_rows, kv_all)


def shards(tokens, w_query, w_key, w_value, w_out, chosen):
    heads = w_query.shape[1] // HEAD_DIM
    kv_heads = w_key.shape[1] // HEAD_DIM
    group = heads // kv_heads
    mine = lax.axis_index("tp")
    my_index = lax.axis_index("kv")
    swap = [(0, 1), (1, 0)]

    own = tokens[0]
    half = own.shape[0]
    count = 2 * half
    peer = lax.ppermute(own, "tp", swap)

    row = jnp.arange(count, dtype=jnp.int32)
    positions = my_index * count + (row + mine * half) % count
    cosine, sine = rotary_tables(positions)

    kv_own = pl.pallas_call(
        kv_kernel,
        out_shape=jax.ShapeDtypeStruct((count, 2 * LANES), jnp.bfloat16),
        name="project_kv",
    )(own, peer, w_key, w_value, cosine, sine)
    local_blocks = count // BLK
    kv_all = lax.all_gather(
        kv_own.reshape(local_blocks, BLK, 2 * LANES), "kv", axis=0, tiled=True
    )

    wq = w_query.reshape(-1, kv_heads, group, HEAD_DIM).transpose(0, 2, 1, 3)
    wq = wq.reshape(w_query.shape)
    wo = w_out.reshape(kv_heads, group, HEAD_DIM, -1).transpose(1, 0, 2, 3)
    wo = wo.reshape(w_out.shape)
    wo_peer = lax.ppermute(wo, "tp", swap)
    queries = pl.pallas_call(
        q_kernel,
        out_shape=jax.ShapeDtypeStruct((count, w_query.shape[1]), jnp.bfloat16),
        name="project_q",
    )(own, peer, wq, cosine, sine)

    flip = mine * (local_blocks // 2)
    picks = chosen[0]
    usable = jnp.concatenate(
        [(picks >= 0).astype(jnp.int32), jnp.ones((local_blocks, 1), jnp.int32)], axis=1
    )
    own_block = my_index * local_blocks + jnp.arange(local_blocks, dtype=jnp.int32)
    blocks = jnp.concatenate([jnp.maximum(picks, 0), own_block[:, None]], axis=1)
    slots = blocks // local_blocks * local_blocks + (blocks + flip) % local_blocks
    half_blocks = local_blocks // 2
    first = mine * half_blocks
    second = half_blocks - first

    def piece(x, start):
        return lax.dynamic_slice_in_dim(x, start, half_blocks, 0)

    att_peer, lse_peer = attend(queries[half:], kv_all, piece(slots, second), piece(usable, second))
    arrived = lax.ppermute(att_peer, "tp", swap)
    att_own, lse_own = attend(queries[:half], kv_all, piece(slots, first), piece(usable, first))
    partial = jnp.dot(att_own, wo, preferred_element_type=jnp.float32)
    normed = pl.pallas_call(
        finish_kernel,
        out_shape=jax.ShapeDtypeStruct((half, wo.shape[1]), jnp.bfloat16),
        name="finish",
    )(partial, arrived, wo_peer)
    lse = jnp.where(
        mine == 0,
        jnp.concatenate([lse_own, lse_peer], axis=0),
        jnp.concatenate([lse_peer, lse_own], axis=0),
    )
    return (normed[None], lse[None])


def solution(mesh):
    placed = (
        P("dp", ("kv", "tp"), None),
        P(None, "tp"),
        P(None, "tp"),
        P(None, "tp"),
        P("tp", None),
        P("dp", "kv", None),
    )
    return jax.shard_map(
        shards,
        mesh=mesh,
        in_specs=placed,
        out_specs=(P("dp", ("kv", "tp"), None), P("dp", "kv", "tp")),
        check_vma=False,
    )
```

```python
import functools

import jax
import jax.numpy as jnp
from jax import lax
from jax.experimental import pallas as pl
from jax.experimental.pallas import tpu as pltpu
from jax.sharding import PartitionSpec as P

HEAD_DIM = 64
BLK = 64
PICK = 15
THETA_BASE = 10000.0
NEGATIVE = -1e30
EPSILON = 1e-06
LANES = 128
CHIPS = 4
HALF_BLOCKS = 4


def rotary_tables(positions):
    half = HEAD_DIM // 2
    inverse = THETA_BASE ** (-jnp.arange(half, dtype=jnp.float32) / half)
    angles = positions.astype(jnp.float32)[:, None] * inverse[None, :]
    cosine = jnp.cos(angles)
    sine = jnp.sin(angles)
    return (
        jnp.concatenate([cosine] * 4, axis=1),
        jnp.concatenate([-sine, sine, -sine, sine], axis=1),
    )


def rotated(values, cosine, sine):
    lane = lax.broadcasted_iota(jnp.int32, values.shape, 1)
    ahead = pltpu.roll(values, LANES - HEAD_DIM // 2, 1)
    behind = pltpu.roll(values, HEAD_DIM // 2, 1)
    swapped = jnp.where(lane % HEAD_DIM < HEAD_DIM // 2, ahead, behind)
    return values * cosine + swapped * sine


def rounded(x):
    return x.astype(jnp.bfloat16).astype(jnp.float32)


def kv_kernel(where_ref, x_ref, wk_ref, wkp_ref, wv_ref, wvp_ref, cos_ref, sin_ref, *rest):
    outs, held = rest[:-1], rest[-1]
    core, chip = where_ref[0], where_ref[1]
    piece = x_ref[...]
    for side, (wk, wv) in enumerate(((wk_ref, wv_ref), (wkp_ref, wvp_ref))):
        owner = core if side == 0 else 1 - core
        keys = rounded(jnp.dot(piece, wk[...], preferred_element_type=jnp.float32))
        keys = rotated(keys, cos_ref[...], sin_ref[...])
        values = jnp.dot(piece, wv[...], preferred_element_type=jnp.float32)
        for b in range(HALF_BLOCKS):
            rows = slice(b * BLK, (b + 1) * BLK)
            turned = values[rows].T
            for j in range(2):
                cols = slice(j * HEAD_DIM, (j + 1) * HEAD_DIM)
                held[2 * owner + j, b] = jnp.concatenate(
                    [keys[rows, cols], turned[cols]], axis=1
                ).astype(jnp.bfloat16)
    for r in range(CHIPS):
        outs[r][...] = held[lax.rem(chip + r, CHIPS)]


def q_kernel(where_ref, x_ref, wq_ref, wqp_ref, cos_ref, sin_ref, *rest):
    outs, held = rest[:-1], rest[-1]
    core, chip = where_ref[0], where_ref[1]
    piece = x_ref[...]
    for side, wq in enumerate((wq_ref, wqp_ref)):
        owner = core if side == 0 else 1 - core
        for j in range(2):
            for t in range(2):
                cols = slice((2 * j + t) * LANES, (2 * j + t + 1) * LANES)
                tile = rounded(jnp.dot(piece, wq[:, cols], preferred_element_type=jnp.float32))
                tile = rotated(tile, cos_ref[...], sin_ref[...]).astype(jnp.bfloat16)
                held[2 * owner + j, :, t * LANES : (t + 1) * LANES] = tile * jnp.bfloat16(
                    HEAD_DIM**-0.5
                )
    for r in range(CHIPS):
        outs[r][...] = held[lax.rem(chip + r, CHIPS)]


def attend_kernel(shifts, planes, slots_ref, bias_ref, *rest):
    queries = rest[: len(shifts)]
    pieces = rest[len(shifts) : len(shifts) + 4 * planes]
    outs = rest[len(shifts) + 4 * planes : -2]
    held, sem = rest[-2:]

    copies = []
    at = 0
    for f in range(2):
        for d in range(planes):
            for ring in range(2):
                first = ((f * planes + d) * CHIPS + 2 * ring) * HALF_BLOCKS
                copies.append(
                    pltpu.make_async_copy(
                        pieces[at], held.at[pl.ds(first, 2 * HALF_BLOCKS)], sem.at[at]
                    )
                )
                at += 1
    for copy in copies:
        copy.start()
    for copy in copies:
        copy.wait()

    left = lax.broadcasted_iota(jnp.int32, (BLK, LANES), 1) < HEAD_DIM
    key_pos = lax.broadcasted_iota(jnp.int32, (BLK, 4 * BLK), 0)
    query_pos = lax.broadcasted_iota(jnp.int32, (BLK, 4 * BLK), 1) % BLK
    causal = key_pos <= query_pos
    left_row = lax.broadcasted_iota(jnp.int32, (1, LANES), 1) < HEAD_DIM

    def one_block(q_ref, row, start):
        tiles = q_ref[pl.ds(start, BLK), :].astype(jnp.float32)
        heads = []
        for g in range(4):
            tile = tiles[:, (g // 2) * LANES : (g // 2 + 1) * LANES]
            if g % 2 == 1:
                tile = pltpu.roll(tile, HEAD_DIM, 1)
            heads.append(jnp.where(left, tile, 0.0).astype(jnp.bfloat16))
        stacked = jnp.concatenate(heads, axis=0)
        blocks = [held[slots_ref[row, p]] for p in range(PICK + 1)]
        scores = lax.dot_general(
            jnp.concatenate(blocks, axis=0),
            stacked,
            (((1,), (1,)), ((), ())),
            preferred_element_type=jnp.float32,
        )
        parts = [scores[p * BLK : (p + 1) * BLK] + bias_ref[row, p] for p in range(PICK)]
        parts.append(jnp.where(causal, scores[PICK * BLK :], NEGATIVE))
        scores = jnp.concatenate(parts, axis=0)
        top = jnp.max(scores, axis=0, keepdims=True)
        exponent = jnp.exp(scores - top)
        total = jnp.sum(exponent, axis=0, keepdims=True)
        turned = []
        for p in range(0, PICK + 1, 2):
            moved = pltpu.roll(blocks[p].astype(jnp.float32), HEAD_DIM, 1)
            turned.append(
                jnp.where(left, moved, blocks[p + 1].astype(jnp.float32)).astype(jnp.bfloat16)
            )
        mixed = jnp.dot(
            jnp.concatenate(turned, axis=1),
            exponent.astype(jnp.bfloat16),
            preferred_element_type=jnp.float32,
        )
        mixed = mixed * (1.0 / total)
        flat = []
        for t in range(2):
            tile = mixed[:, t * LANES : (t + 1) * LANES].T
            flat.append(jnp.concatenate([tile[:HEAD_DIM], tile[HEAD_DIM:]], axis=1))
        return jnp.concatenate(flat, axis=1).astype(jnp.bfloat16), top + jnp.log(total)

    for n, r in enumerate(shifts):
        q_ref, att_ref, lse_ref = queries[n], outs[2 * n], outs[2 * n + 1]

        def pair(p, carry, q_ref=q_ref, att_ref=att_ref, lse_ref=lse_ref, r=r):
            logs = []
            for u in range(2):
                start = pl.multiple_of((2 * p + u) * BLK, BLK)
                att, log = one_block(q_ref, r * HALF_BLOCKS + 2 * p + u, start)
                att_ref[pl.ds(start, BLK), :] = att
                logs.append(log)
            place = pl.ds(pl.multiple_of(p * LANES, LANES), LANES)
            for t in range(2):
                one = logs[0][:, t * LANES : (t + 1) * LANES]
                two = logs[1][:, t * LANES : (t + 1) * LANES]
                lse_ref[2 * t : 2 * t + 1, place] = jnp.where(
                    left_row, one, pltpu.roll(two, HEAD_DIM, 1)
                )
                lse_ref[2 * t + 1 : 2 * t + 2, place] = jnp.where(
                    left_row, pltpu.roll(one, HEAD_DIM, 1), two
                )
            return carry

        lax.fori_loop(0, HALF_BLOCKS // 2, pair, 0)


def lse_kernel(where_ref, *rest):
    pieces, keep_ref, give_ref, held = rest[:4], rest[4], rest[5], rest[6]
    core, chip = where_ref[0], where_ref[1]
    for r in range(CHIPS):
        held[lax.rem(chip + r, CHIPS)] = pieces[r][...]
    for j in range(2):
        keep_ref[4 * j : 4 * j + 4, :] = held[2 * core + j]
        give_ref[4 * j : 4 * j + 4, :] = held[2 * (1 - core) + j]


def finish_kernel(where_ref, *rest):
    pieces, w_ref, wp_ref, out_ref, held = rest[:4], rest[4], rest[5], rest[6], rest[7]
    core, chip = where_ref[0], where_ref[1]
    for r in range(CHIPS):
        held[lax.rem(chip + r, CHIPS)] = pieces[r][...]
    width = held.shape[2]
    projected = None
    for side, w in enumerate((w_ref, wp_ref)):
        owner = core if side == 0 else 1 - core
        for j in range(2):
            term = jnp.dot(
                held[2 * owner + j],
                w[j * width : (j + 1) * width, :],
                preferred_element_type=jnp.float32,
            )
            projected = term if projected is None else projected + term
    scale = lax.rsqrt(jnp.mean(projected * projected, axis=1, keepdims=True) + EPSILON)
    out_ref[...] = (projected * scale).astype(jnp.bfloat16)


SMEM = pl.BlockSpec(memory_space=pltpu.SMEM)
VMEM = pl.BlockSpec(memory_space=pltpu.VMEM)
ANY = pl.BlockSpec(memory_space=pl.ANY)


def attend(shifts, planes, slots, bias, queries, pieces):
    rows, width = queries[0].shape
    shape = []
    for _ in shifts:
        shape.append(jax.ShapeDtypeStruct((rows, width), jnp.bfloat16))
        shape.append(jax.ShapeDtypeStruct((4, rows), jnp.float32))
    total = 2 * planes * CHIPS * HALF_BLOCKS
    return pl.pallas_call(
        functools.partial(attend_kernel, shifts, planes),
        in_specs=[SMEM, SMEM] + [VMEM] * len(shifts) + [ANY] * len(pieces),
        out_specs=[VMEM] * len(shape),
        out_shape=shape,
        scratch_shapes=[
            pltpu.VMEM((total, BLK, LANES), jnp.bfloat16),
            pltpu.SemaphoreType.DMA((len(pieces),)),
        ],
        cost_estimate=pl.CostEstimate(
            flops=len(shifts) * 4 * rows * width * (PICK + 1) * BLK * 8,
            bytes_accessed=total * BLK * LANES * 2,
            transcendentals=0,
        ),
        name="attend",
    )(slots, bias, *queries, *pieces)


def shards(tokens, w_query, w_key, w_value, w_out, chosen):
    core = lax.axis_index("tp")
    index = lax.axis_index("kv")
    planes = lax.axis_size("kv") // CHIPS
    plane, chip = index // CHIPS, index % CHIPS
    here = jnp.stack([core, chip]).astype(jnp.int32)

    def partner(x):
        return lax.ppermute(x, "tp", [(0, 1), (1, 0)])

    def along_y(x, r):
        return lax.ppermute(
            x,
            "kv",
            [
                (z * CHIPS + y, z * CHIPS + (y + r) % CHIPS)
                for z in range(planes)
                for y in range(CHIPS)
            ],
        )

    def along_z(x, step):
        return lax.ppermute(
            x,
            "kv",
            [
                (z * CHIPS + y, (z + step) % planes * CHIPS + y)
                for z in range(planes)
                for y in range(CHIPS)
            ],
        )

    own = tokens[0]
    rows = own.shape[0]
    wk_peer, wv_peer = partner(w_key), partner(w_value)
    wq_peer, wo_peer = partner(w_query), partner(w_out)

    base = index * 2 * rows + core * rows
    cosine, sine = rotary_tables(base + jnp.arange(rows, dtype=jnp.int32))

    piece_shape = (HALF_BLOCKS, BLK, LANES)
    kv_out = pl.pallas_call(
        kv_kernel,
        in_specs=[SMEM] + [VMEM] * 7,
        out_specs=[VMEM] * CHIPS,
        out_shape=[jax.ShapeDtypeStruct(piece_shape, jnp.bfloat16)] * CHIPS,
        scratch_shapes=[pltpu.VMEM((CHIPS,) + piece_shape, jnp.bfloat16)],
        name="project_kv",
    )(here, own, w_key, wk_peer, w_value, wv_peer, cosine, sine)
    kv_in = [kv_out[0]] + [along_y(kv_out[r], r) for r in range(1, CHIPS)]
    starts = [jnp.stack(kv_in[:2]), jnp.stack(kv_in[2:])]

    q_shape = (rows, 4 * HEAD_DIM)
    q_out = pl.pallas_call(
        q_kernel,
        in_specs=[SMEM] + [VMEM] * 5,
        out_specs=[VMEM] * CHIPS,
        out_shape=[jax.ShapeDtypeStruct(q_shape, jnp.bfloat16)] * CHIPS,
        scratch_shapes=[pltpu.VMEM((CHIPS,) + q_shape, jnp.bfloat16)],
        name="project_q",
    )(here, own, w_query, wq_peer, cosine, sine)
    q_in = [q_out[0]] + [along_y(q_out[r], r) for r in range(1, CHIPS)]

    rings = [{0: starts[0]}, {0: starts[1]}]
    longer, shorter = planes // 2, planes - 1 - planes // 2
    for ring, (ups, downs) in enumerate(((longer, shorter), (shorter, longer))):
        moving = starts[ring]
        for n in range(1, ups + 1):
            moving = along_z(moving, 1)
            rings[ring][n] = moving
        moving = starts[ring]
        for n in range(1, downs + 1):
            moving = along_z(moving, -1)
            rings[ring][planes - n] = moving
    flat = (2 * HALF_BLOCKS, BLK, LANES)
    pieces = [rings[ring][d].reshape(flat) for d in range(planes) for ring in range(2)]
    pieces = pieces + [partner(x) for x in pieces]

    picks_own = lax.dynamic_slice_in_dim(chosen[0], core * HALF_BLOCKS, HALF_BLOCKS, 0)
    picks = jnp.stack([picks_own] + [along_y(picks_own, r) for r in range(1, CHIPS)])
    shift = jnp.arange(CHIPS, dtype=jnp.int32)
    source = (chip - shift) % CHIPS
    own_block = (
        plane * (8 * CHIPS)
        + source[:, None] * 8
        + core * HALF_BLOCKS
        + jnp.arange(HALF_BLOCKS, dtype=jnp.int32)[None, :]
    )
    blocks = jnp.concatenate([picks, own_block[:, :, None]], axis=2)
    bias = jnp.where(blocks >= 0, 0.0, NEGATIVE).astype(jnp.float32)
    blocks = jnp.maximum(blocks, 0)
    flag = (blocks // HALF_BLOCKS % 2) ^ core
    distance = (plane - blocks // (8 * CHIPS)) % planes
    turn = (chip - blocks // 8 % CHIPS) % CHIPS
    slots = ((flag * planes + distance) * CHIPS + turn) * HALF_BLOCKS + blocks % HALF_BLOCKS
    slots = slots.reshape(CHIPS * HALF_BLOCKS, PICK + 1)
    bias = bias.reshape(CHIPS * HALF_BLOCKS, PICK + 1)

    att, lse = {}, {}
    for shifts in ((2, 1), (3, 0)):
        done = attend(shifts, planes, slots, bias, [q_in[r] for r in shifts], pieces)
        for n, r in enumerate(shifts):
            att[r], lse[r] = done[2 * n], done[2 * n + 1]
            if r:
                att[r], lse[r] = along_y(att[r], -r), along_y(lse[r], -r)

    keep, give = pl.pallas_call(
        lse_kernel,
        in_specs=[SMEM] + [VMEM] * CHIPS,
        out_specs=[VMEM] * 2,
        out_shape=[jax.ShapeDtypeStruct((8, rows), jnp.float32)] * 2,
        scratch_shapes=[pltpu.VMEM((CHIPS, 4, rows), jnp.float32)],
        name="sort_logsums",
    )(here, *[lse[r] for r in range(CHIPS)])
    got = partner(give)
    normed = pl.pallas_call(
        finish_kernel,
        in_specs=[SMEM] + [VMEM] * (CHIPS + 2),
        out_specs=VMEM,
        out_shape=jax.ShapeDtypeStruct((rows, w_out.shape[1]), jnp.bfloat16),
        scratch_shapes=[pltpu.VMEM((CHIPS, rows, 4 * HEAD_DIM), jnp.bfloat16)],
        name="finish",
    )(here, *[att[r] for r in range(CHIPS)], w_out, wo_peer)
    first = jnp.where(core == 0, keep, got)
    second = jnp.where(core == 0, got, keep)
    logsums = jnp.concatenate([first, second], axis=1).T
    return (normed[None], logsums[None])


def solution(mesh):
    placed = (
        P("dp", ("kv", "tp"), None),
        P(None, "tp"),
        P(None, "tp"),
        P(None, "tp"),
        P("tp", None),
        P("dp", "kv", None),
    )
    return jax.shard_map(
        shards,
        mesh=mesh,
        in_specs=placed,
        out_specs=(P("dp", ("kv", "tp"), None), P("dp", "kv", "tp")),
        check_vma=False,
    )
```

```python
import functools

import jax
import jax.numpy as jnp
from jax import lax
from jax.experimental import pallas as pl
from jax.experimental.pallas import tpu as pltpu
from jax.sharding import PartitionSpec as P

HEAD_DIM = 64
BLK = 64
PICK = 15
THETA_BASE = 10000.0
NEGATIVE = -1e30
EPSILON = 1e-06
LANES = 128
CHIPS = 4
HALF_BLOCKS = 4
EXTRA = 16


def rotary_tables(positions):
    half = HEAD_DIM // 2
    inverse = THETA_BASE ** (-jnp.arange(half, dtype=jnp.float32) / half)
    angles = positions.astype(jnp.float32)[:, None] * inverse[None, :]
    cosine = jnp.cos(angles)
    sine = jnp.sin(angles)
    return (
        jnp.concatenate([cosine] * 4, axis=1),
        jnp.concatenate([-sine, sine, -sine, sine], axis=1),
    )


def rotated(values, cosine, sine):
    lane = lax.broadcasted_iota(jnp.int32, values.shape, 1)
    ahead = pltpu.roll(values, LANES - HEAD_DIM // 2, 1)
    behind = pltpu.roll(values, HEAD_DIM // 2, 1)
    swapped = jnp.where(lane % HEAD_DIM < HEAD_DIM // 2, ahead, behind)
    return values * cosine + swapped * sine


def rounded(x):
    return x.astype(jnp.bfloat16).astype(jnp.float32)


def kv_kernel(where_ref, x_ref, wk_ref, wkp_ref, wv_ref, wvp_ref, cos_ref, sin_ref, *rest):
    outs, held = rest[:-1], rest[-1]
    core, chip = where_ref[0], where_ref[1]
    piece = x_ref[...]
    for side, (wk, wv) in enumerate(((wk_ref, wv_ref), (wkp_ref, wvp_ref))):
        owner = core if side == 0 else 1 - core
        keys = rounded(jnp.dot(piece, wk[...], preferred_element_type=jnp.float32))
        keys = rotated(keys, cos_ref[...], sin_ref[...])
        values = jnp.dot(piece, wv[...], preferred_element_type=jnp.float32)
        for b in range(HALF_BLOCKS):
            rows = slice(b * BLK, (b + 1) * BLK)
            turned = values[rows].T
            for j in range(2):
                cols = slice(j * HEAD_DIM, (j + 1) * HEAD_DIM)
                held[2 * owner + j, b] = jnp.concatenate(
                    [keys[rows, cols], turned[cols]], axis=1
                ).astype(jnp.bfloat16)
    for r in range(CHIPS):
        outs[r][...] = held[lax.rem(chip + r, CHIPS)]


def q_kernel(where_ref, x_ref, wq_ref, wqp_ref, cos_ref, sin_ref, picks_ref, *rest):
    outs, held = rest[:-1], rest[-1]
    core, chip = where_ref[0], where_ref[1]
    piece = x_ref[...]
    rows = piece.shape[0]
    for side, wq in enumerate((wq_ref, wqp_ref)):
        owner = core if side == 0 else 1 - core
        for j in range(2):
            for t in range(2):
                cols = slice((2 * j + t) * LANES, (2 * j + t + 1) * LANES)
                tile = rounded(jnp.dot(piece, wq[:, cols], preferred_element_type=jnp.float32))
                tile = rotated(tile, cos_ref[...], sin_ref[...]).astype(jnp.bfloat16)
                held[2 * owner + j, :, t * LANES : (t + 1) * LANES] = tile * jnp.bfloat16(
                    HEAD_DIM**-0.5
                )
    mine = jnp.where(core == 0, picks_ref[:HALF_BLOCKS, :], picks_ref[HALF_BLOCKS:, :])
    mine = jnp.concatenate(
        [mine.astype(jnp.float32), jnp.zeros((EXTRA - HALF_BLOCKS, LANES), jnp.float32)], axis=0
    ).astype(jnp.bfloat16)
    for r in range(CHIPS):
        outs[r][:rows, :] = held[lax.rem(chip + r, CHIPS)]
        outs[r][rows:, :LANES] = mine
        outs[r][rows:, LANES:] = jnp.zeros_like(mine)


def attend_kernel(count, planes, slots_ref, bias_ref, *rest):
    queries = rest[:count]
    pieces = rest[count : count + 2 * planes]
    outs = rest[count + 2 * planes : 2 * count + 2 * planes]
    held, asked, told, logs_held, sem = rest[2 * count + 2 * planes :]
    rows = outs[0].shape[0] - EXTRA
    chunk = CHIPS * HALF_BLOCKS

    copies = [
        pltpu.make_async_copy(piece, held.at[pl.ds(n * chunk, chunk)], sem.at[n])
        for n, piece in enumerate(pieces)
    ]
    for copy in copies:
        copy.start()
    for n in range(count):
        asked[n] = queries[n][:rows, :]
    logs_held[...] = jnp.zeros_like(logs_held)
    for copy in copies:
        copy.wait()

    left = lax.broadcasted_iota(jnp.int32, (BLK, LANES), 1) < HEAD_DIM
    key_pos = lax.broadcasted_iota(jnp.int32, (BLK, 4 * BLK), 0)
    query_pos = lax.broadcasted_iota(jnp.int32, (BLK, 4 * BLK), 1) % BLK
    causal = key_pos <= query_pos
    left_row = lax.broadcasted_iota(jnp.int32, (1, LANES), 1) < HEAD_DIM

    def one_block(n, row, start):
        tiles = asked[n, pl.ds(start, BLK), :].astype(jnp.float32)
        heads = []
        for g in range(4):
            tile = tiles[:, (g // 2) * LANES : (g // 2 + 1) * LANES]
            if g % 2 == 1:
                tile = pltpu.roll(tile, HEAD_DIM, 1)
            heads.append(jnp.where(left, tile, 0.0).astype(jnp.bfloat16))
        stacked = jnp.concatenate(heads, axis=0)
        blocks = [held[slots_ref[row, p]] for p in range(PICK + 1)]
        scores = lax.dot_general(
            jnp.concatenate(blocks, axis=0),
            stacked,
            (((1,), (1,)), ((), ())),
            preferred_element_type=jnp.float32,
        )
        parts = [scores[p * BLK : (p + 1) * BLK] + bias_ref[row, p] for p in range(PICK)]
        parts.append(jnp.where(causal, scores[PICK * BLK :], NEGATIVE))
        scores = jnp.concatenate(parts, axis=0)
        top = jnp.max(scores, axis=0, keepdims=True)
        exponent = jnp.exp(scores - top)
        total = jnp.sum(exponent, axis=0, keepdims=True)
        turned = []
        for p in range(0, PICK + 1, 2):
            moved = pltpu.roll(blocks[p].astype(jnp.float32), HEAD_DIM, 1)
            turned.append(
                jnp.where(left, moved, blocks[p + 1].astype(jnp.float32)).astype(jnp.bfloat16)
            )
        mixed = jnp.dot(
            jnp.concatenate(turned, axis=1),
            exponent.astype(jnp.bfloat16),
            preferred_element_type=jnp.float32,
        )
        mixed = mixed * (1.0 / total)
        flat = []
        for t in range(2):
            tile = mixed[:, t * LANES : (t + 1) * LANES].T
            flat.append(jnp.concatenate([tile[:HEAD_DIM], tile[HEAD_DIM:]], axis=1))
        return jnp.concatenate(flat, axis=1).astype(jnp.bfloat16), top + jnp.log(total)

    def pair(step, carry):
        n, p = lax.div(step, HALF_BLOCKS // 2), lax.rem(step, HALF_BLOCKS // 2)
        logs = []
        for u in range(2):
            start = pl.multiple_of((2 * p + u) * BLK, BLK)
            att, log = one_block(n, 2 * step + u, start)
            told[n, pl.ds(start, BLK), :] = att
            logs.append(log)
        place = pl.ds(pl.multiple_of(p * LANES, LANES), LANES)
        for t in range(2):
            one = logs[0][:, t * LANES : (t + 1) * LANES]
            two = logs[1][:, t * LANES : (t + 1) * LANES]
            pieces_of = (
                jnp.where(left_row, one, pltpu.roll(two, HEAD_DIM, 1)),
                jnp.where(left_row, pltpu.roll(one, HEAD_DIM, 1), two),
            )
            for j, log in enumerate(pieces_of):
                head = 2 * t + j
                high = rounded(log)
                middle = rounded(log - high)
                low = log - high - middle
                for k, part in enumerate((high, middle, low)):
                    logs_held[n, 4 * k + head : 4 * k + head + 1, place] = part
        return carry

    lax.fori_loop(0, count * HALF_BLOCKS // 2, pair, 0)
    for n in range(count):
        outs[n][:rows, :] = told[n]
        outs[n][rows:, :] = logs_held[n].astype(jnp.bfloat16)


def lse_kernel(where_ref, *rest):
    pieces, keep_ref, give_ref, held = rest[:4], rest[4], rest[5], rest[6]
    core, chip = where_ref[0], where_ref[1]
    for r in range(CHIPS):
        parts = pieces[r][...].astype(jnp.float32)
        held[lax.rem(chip + r, CHIPS)] = parts[0:4] + parts[4:8] + parts[8:12]
    for j in range(2):
        keep_ref[4 * j : 4 * j + 4, :] = held[2 * core + j]
        give_ref[4 * j : 4 * j + 4, :] = held[2 * (1 - core) + j]


def finish_kernel(where_ref, *rest):
    pieces, w_ref, wp_ref, out_ref, held = rest[:4], rest[4], rest[5], rest[6], rest[7]
    core, chip = where_ref[0], where_ref[1]
    rows, width = held.shape[1:]
    for r in range(CHIPS):
        held[lax.rem(chip + r, CHIPS)] = pieces[r][:rows, :]
    projected = None
    for side, w in enumerate((w_ref, wp_ref)):
        owner = core if side == 0 else 1 - core
        for j in range(2):
            term = jnp.dot(
                held[2 * owner + j],
                w[j * width : (j + 1) * width, :],
                preferred_element_type=jnp.float32,
            )
            projected = term if projected is None else projected + term
    scale = lax.rsqrt(jnp.mean(projected * projected, axis=1, keepdims=True) + EPSILON)
    out_ref[...] = (projected * scale).astype(jnp.bfloat16)


SMEM = pl.BlockSpec(memory_space=pltpu.SMEM)
VMEM = pl.BlockSpec(memory_space=pltpu.VMEM)
ANY = pl.BlockSpec(memory_space=pl.ANY)


def grant(mib):
    return pltpu.CompilerParams(vmem_limit_bytes=mib * 2**20)


def attend(planes, slots, bias, queries, pieces):
    count = len(queries)
    rows, width = queries[0].shape[0] - EXTRA, queries[0].shape[1]
    total = 2 * planes * CHIPS * HALF_BLOCKS
    return pl.pallas_call(
        functools.partial(attend_kernel, count, planes),
        in_specs=[SMEM, SMEM] + [VMEM] * count + [ANY] * len(pieces),
        out_specs=[VMEM] * count,
        out_shape=[jax.ShapeDtypeStruct((rows + EXTRA, width), jnp.bfloat16)] * count,
        scratch_shapes=[
            pltpu.VMEM((total, BLK, LANES), jnp.bfloat16),
            pltpu.VMEM((count, rows, width), jnp.bfloat16),
            pltpu.VMEM((count, rows, width), jnp.bfloat16),
            pltpu.VMEM((count, EXTRA, rows), jnp.float32),
            pltpu.SemaphoreType.DMA((len(pieces),)),
        ],
        cost_estimate=pl.CostEstimate(
            flops=count * 32 * rows * width * (PICK + 1) * BLK,
            bytes_accessed=total * BLK * LANES * 2,
            transcendentals=0,
        ),
        compiler_params=grant(16),
        name="attend",
    )(slots, bias, *queries, *pieces)


def tied(value, *others):
    return lax.optimization_barrier((value,) + others)[0]


def shards(tokens, w_query, w_key, w_value, w_out, chosen):
    core = lax.axis_index("tp")
    index = lax.axis_index("kv")
    planes = lax.axis_size("kv") // CHIPS
    plane, chip = index // CHIPS, index % CHIPS
    here = jnp.stack([core, chip]).astype(jnp.int32)

    def partner(x):
        return lax.ppermute(x, "tp", [(0, 1), (1, 0)])

    def along_y(x, r):
        return lax.ppermute(
            x,
            "kv",
            [
                (z * CHIPS + y, z * CHIPS + (y + r) % CHIPS)
                for z in range(planes)
                for y in range(CHIPS)
            ],
        )

    def along_z(x, step):
        return lax.ppermute(
            x,
            "kv",
            [
                (z * CHIPS + y, (z + step) % planes * CHIPS + y)
                for z in range(planes)
                for y in range(CHIPS)
            ],
        )

    own = tokens[0]
    rows = own.shape[0]
    wk_peer, wv_peer = partner(w_key), partner(w_value)
    wq_peer = partner(tied(w_query, wk_peer, wv_peer))

    base = index * 2 * rows + core * rows
    cosine, sine = rotary_tables(base + jnp.arange(rows, dtype=jnp.int32))

    piece_shape = (HALF_BLOCKS, BLK, LANES)
    kv_out = pl.pallas_call(
        kv_kernel,
        in_specs=[SMEM] + [VMEM] * 7,
        out_specs=[VMEM] * CHIPS,
        out_shape=[jax.ShapeDtypeStruct(piece_shape, jnp.bfloat16)] * CHIPS,
        scratch_shapes=[pltpu.VMEM((CHIPS,) + piece_shape, jnp.bfloat16)],
        compiler_params=grant(8),
        name="project_kv",
    )(here, own, w_key, wk_peer, w_value, wv_peer, cosine, sine)
    kv_in = [kv_out[0]] + [along_y(kv_out[r], r) for r in range(1, CHIPS)]

    q_shape = (rows + EXTRA, 4 * HEAD_DIM)
    q_out = pl.pallas_call(
        q_kernel,
        in_specs=[SMEM] + [VMEM] * 6,
        out_specs=[VMEM] * CHIPS,
        out_shape=[jax.ShapeDtypeStruct(q_shape, jnp.bfloat16)] * CHIPS,
        scratch_shapes=[pltpu.VMEM((CHIPS, rows, 4 * HEAD_DIM), jnp.bfloat16)],
        compiler_params=grant(10),
        name="project_q",
    )(
        here,
        own,
        w_query,
        wq_peer,
        tied(cosine, kv_out[0]),
        sine,
        jnp.pad(chosen[0], ((0, 0), (0, LANES - PICK))),
    )
    start = jnp.stack(kv_in)

    chunks = {0: start}
    order = [0]
    up = down = start
    for n in range(1, planes // 2 + 1):
        up = along_z(up, 1)
        chunks[n] = up
        order.append(n)
        if n <= planes - 1 - planes // 2:
            down = along_z(down, -1)
            chunks[planes - n] = down
            order.append(planes - n)
    q_ready = [tied(q_out[r], chunks[1]) for r in range(CHIPS)]
    q_in = [q_ready[0]] + [along_y(q_ready[r], r) for r in range(1, CHIPS)]
    wo_peer = partner(tied(w_out, chunks[1]))

    flat = (CHIPS * HALF_BLOCKS, BLK, LANES)
    swapped = {}
    for at, d in enumerate(order):
        later = order[min(at + 2, len(order) - 1)]
        value = chunks[d] if later == d else tied(chunks[d], chunks[later])
        swapped[d] = partner(value)
    pieces = [chunks[d].reshape(flat) for d in range(planes)]
    pieces += [swapped[d].reshape(flat) for d in range(planes)]

    picks = jnp.stack([q[rows : rows + HALF_BLOCKS, :PICK] for q in q_in]).astype(jnp.int32)
    shift = jnp.arange(CHIPS, dtype=jnp.int32)
    source = (chip - shift) % CHIPS
    own_block = (
        plane * (8 * CHIPS)
        + source[:, None] * 8
        + core * HALF_BLOCKS
        + jnp.arange(HALF_BLOCKS, dtype=jnp.int32)[None, :]
    )
    blocks = jnp.concatenate([picks, own_block[:, :, None]], axis=2)
    bias = jnp.where(blocks >= 0, 0.0, NEGATIVE).astype(jnp.float32)
    blocks = jnp.maximum(blocks, 0)
    flag = (blocks // HALF_BLOCKS % 2) ^ core
    distance = (plane - blocks // (8 * CHIPS)) % planes
    turn = (chip - blocks // 8 % CHIPS) % CHIPS
    slots = ((flag * planes + distance) * CHIPS + turn) * HALF_BLOCKS + blocks % HALF_BLOCKS

    att = {}
    for shifts in ((2, 1, 3), (0,)):
        span = slice(1, None) if len(shifts) > 1 else slice(0, 1)
        names = sorted(shifts)
        done = attend(
            planes,
            slots[span].reshape(-1, PICK + 1),
            bias[span].reshape(-1, PICK + 1),
            [q_in[r] for r in names],
            pieces,
        )
        for n, r in enumerate(names):
            att[r] = along_y(done[n], -r) if r else done[n]

    tail = rows // EXTRA
    keep, give = pl.pallas_call(
        lse_kernel,
        grid=(1,),
        in_specs=[SMEM] + [pl.BlockSpec((EXTRA, rows), lambda i: (tail, 0))] * CHIPS,
        out_specs=[pl.BlockSpec((8, rows), lambda i: (0, 0))] * 2,
        out_shape=[jax.ShapeDtypeStruct((8, rows), jnp.float32)] * 2,
        scratch_shapes=[pltpu.VMEM((CHIPS, 4, rows), jnp.float32)],
        compiler_params=grant(4),
        name="sort_logsums",
    )(here, *[att[r] for r in range(CHIPS)])
    got = partner(give)
    normed = pl.pallas_call(
        finish_kernel,
        in_specs=[SMEM] + [VMEM] * (CHIPS + 2),
        out_specs=VMEM,
        out_shape=jax.ShapeDtypeStruct((rows, w_out.shape[1]), jnp.bfloat16),
        scratch_shapes=[pltpu.VMEM((CHIPS, rows, 4 * HEAD_DIM), jnp.bfloat16)],
        compiler_params=grant(10),
        name="finish",
    )(here, *[att[r] for r in range(CHIPS)], w_out, wo_peer)
    first = jnp.where(core == 0, keep, got)
    second = jnp.where(core == 0, got, keep)
    logsums = jnp.concatenate([first, second], axis=1).T
    return (normed[None], logsums[None])


def solution(mesh):
    placed = (
        P("dp", ("kv", "tp"), None),
        P(None, "tp"),
        P(None, "tp"),
        P(None, "tp"),
        P("tp", None),
        P("dp", "kv", None),
    )
    return jax.shard_map(
        shards,
        mesh=mesh,
        in_specs=placed,
        out_specs=(P("dp", ("kv", "tp"), None), P("dp", "kv", "tp")),
        check_vma=False,
    )
```

```python
import functools

import jax
import jax.numpy as jnp
from jax import lax
from jax.experimental import pallas as pl
from jax.experimental.pallas import tpu as pltpu
from jax.sharding import PartitionSpec as P

HEAD_DIM = 64
BLK = 64
PICK = 15
THETA_BASE = 10000.0
NEGATIVE = -1e30
EPSILON = 1e-06
LANES = 128
CHIPS = 4
HALF_BLOCKS = 4
EXTRA = 16


def rotary_tables(positions):
    half = HEAD_DIM // 2
    inverse = THETA_BASE ** (-jnp.arange(half, dtype=jnp.float32) / half)
    angles = positions.astype(jnp.float32)[:, None] * inverse[None, :]
    cosine = jnp.cos(angles)
    sine = jnp.sin(angles)
    return (
        jnp.concatenate([cosine] * 4, axis=1),
        jnp.concatenate([-sine, sine, -sine, sine], axis=1),
    )


def rotated(values, cosine, sine):
    lane = lax.broadcasted_iota(jnp.int32, values.shape, 1)
    ahead = pltpu.roll(values, LANES - HEAD_DIM // 2, 1)
    behind = pltpu.roll(values, HEAD_DIM // 2, 1)
    swapped = jnp.where(lane % HEAD_DIM < HEAD_DIM // 2, ahead, behind)
    return values * cosine + swapped * sine


def rounded(x):
    return x.astype(jnp.bfloat16).astype(jnp.float32)


def kv_kernel(where_ref, x_ref, wk_ref, wkp_ref, wv_ref, wvp_ref, cos_ref, sin_ref, *rest):
    outs, held = rest[:-1], rest[-1]
    core, chip = where_ref[0], where_ref[1]
    piece = x_ref[...]
    for side, (wk, wv) in enumerate(((wk_ref, wv_ref), (wkp_ref, wvp_ref))):
        owner = core if side == 0 else 1 - core
        keys = rounded(jnp.dot(piece, wk[...], preferred_element_type=jnp.float32))
        keys = rotated(keys, cos_ref[...], sin_ref[...])
        values = jnp.dot(piece, wv[...], preferred_element_type=jnp.float32)
        for b in range(HALF_BLOCKS):
            rows = slice(b * BLK, (b + 1) * BLK)
            turned = values[rows].T
            for j in range(2):
                cols = slice(j * HEAD_DIM, (j + 1) * HEAD_DIM)
                held[2 * owner + j, b] = jnp.concatenate(
                    [keys[rows, cols], turned[cols]], axis=1
                ).astype(jnp.bfloat16)
    for r in range(CHIPS):
        outs[r][...] = held[lax.rem(chip + r, CHIPS)]


def q_kernel(where_ref, x_ref, wq_ref, wqp_ref, cos_ref, sin_ref, picks_ref, *rest):
    outs, held = rest[:-1], rest[-1]
    core, chip = where_ref[0], where_ref[1]
    piece = x_ref[...]
    rows = piece.shape[0]
    for side, wq in enumerate((wq_ref, wqp_ref)):
        owner = core if side == 0 else 1 - core
        for j in range(2):
            for t in range(2):
                cols = slice((2 * j + t) * LANES, (2 * j + t + 1) * LANES)
                tile = rounded(jnp.dot(piece, wq[:, cols], preferred_element_type=jnp.float32))
                tile = rotated(tile, cos_ref[...], sin_ref[...]).astype(jnp.bfloat16)
                held[2 * owner + j, :, t * LANES : (t + 1) * LANES] = tile * jnp.bfloat16(
                    HEAD_DIM**-0.5
                )
    mine = jnp.where(core == 0, picks_ref[:HALF_BLOCKS, :], picks_ref[HALF_BLOCKS:, :])
    mine = jnp.concatenate(
        [mine.astype(jnp.float32), jnp.zeros((EXTRA - HALF_BLOCKS, LANES), jnp.float32)], axis=0
    ).astype(jnp.bfloat16)
    for r in range(CHIPS):
        outs[r][:rows, :] = held[lax.rem(chip + r, CHIPS)]
        outs[r][rows:, :LANES] = mine
        outs[r][rows:, LANES:] = jnp.zeros_like(mine)


def assemble_kernel(places, resumed, *refs):
    pieces = refs[: len(places)]
    out_ref, sem = refs[-2:]
    chunk = CHIPS * HALF_BLOCKS
    copies = [
        pltpu.make_async_copy(piece, out_ref.at[pl.ds(place * chunk, chunk)], sem.at[n])
        for n, (piece, place) in enumerate(zip(pieces, places))
    ]
    for copy in copies:
        copy.start()
    for copy in copies:
        copy.wait()


def attend_kernel(slots_ref, bias_ref, q_ref, held, out_ref, logs_held):
    rows = out_ref.shape[0] - EXTRA
    logs_held[...] = jnp.zeros_like(logs_held)

    left = lax.broadcasted_iota(jnp.int32, (BLK, LANES), 1) < HEAD_DIM
    key_pos = lax.broadcasted_iota(jnp.int32, (BLK, 4 * BLK), 0)
    query_pos = lax.broadcasted_iota(jnp.int32, (BLK, 4 * BLK), 1) % BLK
    causal = key_pos <= query_pos
    left_row = lax.broadcasted_iota(jnp.int32, (1, LANES), 1) < HEAD_DIM

    def one_block(row, start):
        tiles = q_ref[pl.ds(start, BLK), :].astype(jnp.float32)
        heads = []
        for g in range(4):
            tile = tiles[:, (g // 2) * LANES : (g // 2 + 1) * LANES]
            if g % 2 == 1:
                tile = pltpu.roll(tile, HEAD_DIM, 1)
            heads.append(jnp.where(left, tile, 0.0).astype(jnp.bfloat16))
        stacked = jnp.concatenate(heads, axis=0)
        blocks = [held[slots_ref[row, p]] for p in range(PICK + 1)]
        scores = lax.dot_general(
            jnp.concatenate(blocks, axis=0),
            stacked,
            (((1,), (1,)), ((), ())),
            preferred_element_type=jnp.float32,
        )
        parts = [scores[p * BLK : (p + 1) * BLK] + bias_ref[row, p] for p in range(PICK)]
        parts.append(jnp.where(causal, scores[PICK * BLK :], NEGATIVE))
        scores = jnp.concatenate(parts, axis=0)
        top = jnp.max(scores, axis=0, keepdims=True)
        exponent = jnp.exp(scores - top)
        total = jnp.sum(exponent, axis=0, keepdims=True)
        turned = []
        for p in range(0, PICK + 1, 2):
            moved = pltpu.roll(blocks[p].astype(jnp.float32), HEAD_DIM, 1)
            turned.append(
                jnp.where(left, moved, blocks[p + 1].astype(jnp.float32)).astype(jnp.bfloat16)
            )
        mixed = jnp.dot(
            jnp.concatenate(turned, axis=1),
            exponent.astype(jnp.bfloat16),
            preferred_element_type=jnp.float32,
        )
        mixed = mixed * (1.0 / total)
        flat = []
        for t in range(2):
            tile = mixed[:, t * LANES : (t + 1) * LANES].T
            flat.append(jnp.concatenate([tile[:HEAD_DIM], tile[HEAD_DIM:]], axis=1))
        return jnp.concatenate(flat, axis=1).astype(jnp.bfloat16), top + jnp.log(total)

    def pair(p, carry):
        logs = []
        for u in range(2):
            start = pl.multiple_of((2 * p + u) * BLK, BLK)
            att, log = one_block(2 * p + u, start)
            out_ref[pl.ds(start, BLK), :] = att
            logs.append(log)
        place = pl.ds(pl.multiple_of(p * LANES, LANES), LANES)
        for t in range(2):
            one = logs[0][:, t * LANES : (t + 1) * LANES]
            two = logs[1][:, t * LANES : (t + 1) * LANES]
            pieces_of = (
                jnp.where(left_row, one, pltpu.roll(two, HEAD_DIM, 1)),
                jnp.where(left_row, pltpu.roll(one, HEAD_DIM, 1), two),
            )
            for j, log in enumerate(pieces_of):
                head = 2 * t + j
                high = rounded(log)
                middle = rounded(log - high)
                low = log - high - middle
                for k, part in enumerate((high, middle, low)):
                    logs_held[4 * k + head : 4 * k + head + 1, place] = part
        return carry

    lax.fori_loop(0, HALF_BLOCKS // 2, pair, 0)
    out_ref[rows:, :] = logs_held[...].astype(jnp.bfloat16)


def lse_kernel(where_ref, *rest):
    pieces, keep_ref, give_ref, held = rest[:4], rest[4], rest[5], rest[6]
    core, chip = where_ref[0], where_ref[1]
    for r in range(CHIPS):
        parts = pieces[r][...].astype(jnp.float32)
        held[lax.rem(chip + r, CHIPS)] = parts[0:4] + parts[4:8] + parts[8:12]
    for j in range(2):
        keep_ref[4 * j : 4 * j + 4, :] = held[2 * core + j]
        give_ref[4 * j : 4 * j + 4, :] = held[2 * (1 - core) + j]


def finish_kernel(where_ref, *rest):
    pieces, w_ref, wp_ref, out_ref, held = rest[:4], rest[4], rest[5], rest[6], rest[7]
    core, chip = where_ref[0], where_ref[1]
    rows, width = held.shape[1:]
    for r in range(CHIPS):
        held[lax.rem(chip + r, CHIPS)] = pieces[r][:rows, :]
    projected = None
    for side, w in enumerate((w_ref, wp_ref)):
        owner = core if side == 0 else 1 - core
        for j in range(2):
            term = jnp.dot(
                held[2 * owner + j],
                w[j * width : (j + 1) * width, :],
                preferred_element_type=jnp.float32,
            )
            projected = term if projected is None else projected + term
    scale = lax.rsqrt(jnp.mean(projected * projected, axis=1, keepdims=True) + EPSILON)
    out_ref[...] = (projected * scale).astype(jnp.bfloat16)


SMEM = pl.BlockSpec(memory_space=pltpu.SMEM)
VMEM = pl.BlockSpec(memory_space=pltpu.VMEM)
ANY = pl.BlockSpec(memory_space=pl.ANY)


def grant(mib):
    return pltpu.CompilerParams(vmem_limit_bytes=mib * 2**20)


def assemble(pieces, places, total, before=None):
    chunk_bytes = CHIPS * HALF_BLOCKS * BLK * LANES * 2
    resumed = before is not None
    return pl.pallas_call(
        functools.partial(assemble_kernel, places, resumed),
        in_specs=[ANY] * (len(pieces) + resumed),
        out_specs=ANY,
        out_shape=pltpu.VMEM((total, BLK, LANES), jnp.bfloat16),
        scratch_shapes=[pltpu.SemaphoreType.DMA((len(pieces),))],
        input_output_aliases={len(pieces): 0} if resumed else {},
        cost_estimate=pl.CostEstimate(
            flops=len(pieces) * chunk_bytes * 500,
            bytes_accessed=2 * len(pieces) * chunk_bytes,
            transcendentals=0,
        ),
        compiler_params=grant(8),
        name="assemble",
    )(*pieces, *([before] if resumed else []))


def attend(slots, bias, queries, held):
    rows, width = queries.shape[0] - EXTRA, queries.shape[1]
    return pl.pallas_call(
        attend_kernel,
        in_specs=[SMEM, SMEM, VMEM, VMEM],
        out_specs=VMEM,
        out_shape=jax.ShapeDtypeStruct((rows + EXTRA, width), jnp.bfloat16),
        scratch_shapes=[pltpu.VMEM((EXTRA, rows), jnp.float32)],
        cost_estimate=pl.CostEstimate(
            flops=32 * rows * width * (PICK + 1) * BLK,
            bytes_accessed=rows * (PICK + 1) * LANES * 2,
            transcendentals=0,
        ),
        compiler_params=grant(16),
        name="attend",
    )(slots, bias, queries, held)


def tied(value, *others):
    return lax.optimization_barrier((value,) + others)[0]


def shards(tokens, w_query, w_key, w_value, w_out, chosen):
    core = lax.axis_index("tp")
    index = lax.axis_index("kv")
    planes = lax.axis_size("kv") // CHIPS
    plane, chip = index // CHIPS, index % CHIPS
    here = jnp.stack([core, chip]).astype(jnp.int32)

    def partner(x):
        return lax.ppermute(x, "tp", [(0, 1), (1, 0)])

    def along_y(x, r):
        return lax.ppermute(
            x,
            "kv",
            [
                (z * CHIPS + y, z * CHIPS + (y + r) % CHIPS)
                for z in range(planes)
                for y in range(CHIPS)
            ],
        )

    def along_z(x, step):
        return lax.ppermute(
            x,
            "kv",
            [
                (z * CHIPS + y, (z + step) % planes * CHIPS + y)
                for z in range(planes)
                for y in range(CHIPS)
            ],
        )

    own = tokens[0]
    rows = own.shape[0]
    wk_peer, wv_peer = partner(w_key), partner(w_value)
    wq_peer = partner(tied(w_query, wk_peer, wv_peer))

    base = index * 2 * rows + core * rows
    cosine, sine = rotary_tables(base + jnp.arange(rows, dtype=jnp.int32))

    piece_shape = (HALF_BLOCKS, BLK, LANES)
    kv_out = pl.pallas_call(
        kv_kernel,
        in_specs=[SMEM] + [VMEM] * 7,
        out_specs=[VMEM] * CHIPS,
        out_shape=[jax.ShapeDtypeStruct(piece_shape, jnp.bfloat16)] * CHIPS,
        scratch_shapes=[pltpu.VMEM((CHIPS,) + piece_shape, jnp.bfloat16)],
        compiler_params=grant(8),
        name="project_kv",
    )(here, own, w_key, wk_peer, w_value, wv_peer, cosine, sine)
    kv_in = [kv_out[0]] + [along_y(kv_out[r], r) for r in range(1, CHIPS)]

    q_shape = (rows + EXTRA, 4 * HEAD_DIM)
    q_out = pl.pallas_call(
        q_kernel,
        in_specs=[SMEM] + [VMEM] * 6,
        out_specs=[VMEM] * CHIPS,
        out_shape=[jax.ShapeDtypeStruct(q_shape, jnp.bfloat16)] * CHIPS,
        scratch_shapes=[pltpu.VMEM((CHIPS, rows, 4 * HEAD_DIM), jnp.bfloat16)],
        compiler_params=grant(10),
        name="project_q",
    )(
        here,
        own,
        w_query,
        wq_peer,
        tied(cosine, kv_out[0]),
        sine,
        jnp.pad(chosen[0], ((0, 0), (0, LANES - PICK))),
    )
    start = jnp.stack(kv_in)

    last = planes // 2
    chunks, swapped = {0: start}, {}
    up = down = start
    q_in = [q_out[0]]
    wo_peer = None
    for n in range(1, last + 1):
        if n == 2:
            up, down, *q_ready = lax.optimization_barrier((up, down) + tuple(q_out))
            q_in = [q_ready[0]] + [along_y(q_ready[r], r) for r in range(1, CHIPS)]
            wo_peer = partner(tied(w_out, up))
            swapped[0] = partner(tied(start, up))
        if n == 3:
            near, far = tied(chunks[1], up), tied(chunks[planes - 1], up)
            up, down, swapped[0] = lax.optimization_barrier((up, down, swapped[0]))
            swapped[1], swapped[planes - 1] = partner(near), partner(far)
        if n == last and n > 2:
            up, *rest = lax.optimization_barrier(
                (up, wo_peer, swapped[1], swapped[planes - 1]) + tuple(q_in)
            )
            wo_peer, swapped[1], swapped[planes - 1] = rest[:3]
            q_in = rest[3:]
        up = along_z(up, 1)
        chunks[n] = up
        if n < last:
            down = along_z(down, -1)
            chunks[planes - n] = down
    if last < 2:
        q_in = [q_out[0]] + [along_y(q_out[r], r) for r in range(1, CHIPS)]
        wo_peer = partner(w_out)
    for d in range(planes):
        if d not in swapped and d != last:
            swapped[d] = partner(chunks[d])

    flat = (CHIPS * HALF_BLOCKS, BLK, LANES)
    total = 2 * planes * CHIPS * HALF_BLOCKS
    early = [d for d in range(planes) if d != last]
    held = assemble(
        [chunks[d].reshape(flat) for d in early] + [swapped[d].reshape(flat) for d in early],
        early + [planes + d for d in early],
        total,
    )
    swapped[last] = partner(chunks[last])
    held = assemble(
        [chunks[last].reshape(flat), swapped[last].reshape(flat)],
        [last, planes + last],
        total,
        held,
    )

    picks = jnp.stack([q[rows : rows + HALF_BLOCKS, :PICK] for q in q_in]).astype(jnp.int32)
    shift = jnp.arange(CHIPS, dtype=jnp.int32)
    source = (chip - shift) % CHIPS
    own_block = (
        plane * (8 * CHIPS)
        + source[:, None] * 8
        + core * HALF_BLOCKS
        + jnp.arange(HALF_BLOCKS, dtype=jnp.int32)[None, :]
    )
    blocks = jnp.concatenate([picks, own_block[:, :, None]], axis=2)
    bias = jnp.where(blocks >= 0, 0.0, NEGATIVE).astype(jnp.float32)
    blocks = jnp.maximum(blocks, 0)
    flag = (blocks // HALF_BLOCKS % 2) ^ core
    distance = (plane - blocks // (8 * CHIPS)) % planes
    turn = (chip - blocks // 8 % CHIPS) % CHIPS
    slots = ((flag * planes + distance) * CHIPS + turn) * HALF_BLOCKS + blocks % HALF_BLOCKS

    att = {}
    for r in (2, 1, 3, 0):
        done = attend(slots[r], bias[r], q_in[r], held)
        att[r] = along_y(done, -r) if r else done

    tail = rows // EXTRA
    keep, give = pl.pallas_call(
        lse_kernel,
        grid=(1,),
        in_specs=[SMEM] + [pl.BlockSpec((EXTRA, rows), lambda i: (tail, 0))] * CHIPS,
        out_specs=[pl.BlockSpec((8, rows), lambda i: (0, 0))] * 2,
        out_shape=[jax.ShapeDtypeStruct((8, rows), jnp.float32)] * 2,
        scratch_shapes=[pltpu.VMEM((CHIPS, 4, rows), jnp.float32)],
        compiler_params=grant(4),
        name="sort_logsums",
    )(here, *[att[r] for r in range(CHIPS)])
    got = partner(give)
    normed = pl.pallas_call(
        finish_kernel,
        in_specs=[SMEM] + [VMEM] * (CHIPS + 2),
        out_specs=VMEM,
        out_shape=jax.ShapeDtypeStruct((rows, w_out.shape[1]), jnp.bfloat16),
        scratch_shapes=[pltpu.VMEM((CHIPS, rows, 4 * HEAD_DIM), jnp.bfloat16)],
        compiler_params=grant(10),
        name="finish",
    )(here, *[att[r] for r in range(CHIPS)], w_out, wo_peer)
    first = jnp.where(core == 0, keep, got)
    second = jnp.where(core == 0, got, keep)
    logsums = jnp.concatenate([first, second], axis=1).T
    return (normed[None], logsums[None])


def solution(mesh):
    placed = (
        P("dp", ("kv", "tp"), None),
        P(None, "tp"),
        P(None, "tp"),
        P(None, "tp"),
        P("tp", None),
        P("dp", "kv", None),
    )
    return jax.shard_map(
        shards,
        mesh=mesh,
        in_specs=placed,
        out_specs=(P("dp", ("kv", "tp"), None), P("dp", "kv", "tp")),
        check_vma=False,
    )
```

```python
import functools

import jax
import jax.numpy as jnp
from jax import lax
from jax.experimental import pallas as pl
from jax.experimental.pallas import tpu as pltpu
from jax.sharding import PartitionSpec as P

HEAD_DIM = 64
BLK = 64
PICK = 15
THETA_BASE = 10000.0
NEGATIVE = -1e30
EPSILON = 1e-06
LANES = 128
CHIPS = 4
HALF_BLOCKS = 4
CHUNK = 4
EXTRA = 16


def rotary_tables(positions):
    half = HEAD_DIM // 2
    inverse = THETA_BASE ** (-jnp.arange(half, dtype=jnp.float32) / half)
    angles = positions.astype(jnp.float32)[:, None] * inverse[None, :]
    cosine = jnp.cos(angles)
    sine = jnp.sin(angles)
    return (
        jnp.concatenate([cosine] * 4, axis=1),
        jnp.concatenate([-sine, sine, -sine, sine], axis=1),
    )


def rotated(values, cosine, sine):
    lane = lax.broadcasted_iota(jnp.int32, values.shape, 1)
    ahead = pltpu.roll(values, LANES - HEAD_DIM // 2, 1)
    behind = pltpu.roll(values, HEAD_DIM // 2, 1)
    swapped = jnp.where(lane % HEAD_DIM < HEAD_DIM // 2, ahead, behind)
    return values * cosine + swapped * sine


def rounded(x):
    return x.astype(jnp.bfloat16).astype(jnp.float32)


def fetch_all(pairs, sems):
    copies = [
        pltpu.make_async_copy(src, dst, sems.at[n]) for n, (src, dst) in enumerate(pairs)
    ]
    for copy in copies:
        copy.start()
    return copies


def kv_kernel(where_ref, x_hbm, wk_hbm, wv_hbm, wkp_ref, wvp_ref, cos_ref, sin_ref, *rest):
    outs, (x_ref, wk_ref, wv_ref, held, sems) = rest[:CHIPS], rest[CHIPS:]
    copies = fetch_all([(x_hbm, x_ref), (wk_hbm, wk_ref), (wv_hbm, wv_ref)], sems)
    core, chip = where_ref[0], where_ref[1]
    for copy in copies:
        copy.wait()
    piece = x_ref[...]
    for side, (wk, wv) in enumerate(((wk_ref, wv_ref), (wkp_ref, wvp_ref))):
        owner = core if side == 0 else 1 - core
        keys = rounded(jnp.dot(piece, wk[...], preferred_element_type=jnp.float32))
        keys = rotated(keys, cos_ref[...], sin_ref[...])
        values = jnp.dot(piece, wv[...], preferred_element_type=jnp.float32)
        for b in range(HALF_BLOCKS):
            rows = slice(b * BLK, (b + 1) * BLK)
            turned = values[rows].T
            for j in range(2):
                cols = slice(j * HEAD_DIM, (j + 1) * HEAD_DIM)
                held[2 * owner + j, b] = jnp.concatenate(
                    [keys[rows, cols], turned[cols]], axis=1
                ).astype(jnp.bfloat16)
    for r in range(CHIPS):
        outs[r][...] = held[lax.rem(chip + r, CHIPS)]


def q_kernel(where_ref, x_hbm, wq_hbm, wqp_ref, cos_ref, sin_ref, picks_ref, *rest):
    outs, (x_ref, wq_ref, held, sems) = rest[:CHIPS], rest[CHIPS:]
    copies = fetch_all([(x_hbm, x_ref), (wq_hbm, wq_ref)], sems)
    core, chip = where_ref[0], where_ref[1]
    rows = x_ref.shape[0]
    for copy in copies:
        copy.wait()
    piece = x_ref[...]
    for side, wq in enumerate((wq_ref, wqp_ref)):
        owner = core if side == 0 else 1 - core
        for j in range(2):
            for t in range(2):
                cols = slice((2 * j + t) * LANES, (2 * j + t + 1) * LANES)
                tile = rounded(jnp.dot(piece, wq[:, cols], preferred_element_type=jnp.float32))
                tile = rotated(tile, cos_ref[...], sin_ref[...]).astype(jnp.bfloat16)
                held[2 * owner + j, :, t * LANES : (t + 1) * LANES] = tile * jnp.bfloat16(
                    HEAD_DIM**-0.5
                )
    mine = jnp.where(core == 0, picks_ref[:HALF_BLOCKS, :], picks_ref[HALF_BLOCKS:, :])
    mine = jnp.concatenate(
        [mine.astype(jnp.float32), jnp.zeros((EXTRA - HALF_BLOCKS, LANES), jnp.float32)], axis=0
    ).astype(jnp.bfloat16)
    for r in range(CHIPS):
        outs[r][:rows, :] = held[lax.rem(chip + r, CHIPS)]
        outs[r][rows:, :LANES] = mine
        outs[r][rows:, LANES:] = jnp.zeros_like(mine)


def assemble_kernel(places, *refs):
    pieces = refs[: len(places)]
    out_ref, sems = refs[-2:]
    copies = fetch_all(
        [
            (piece, out_ref.at[pl.ds(place, piece.shape[0])])
            for piece, place in zip(pieces, places)
        ],
        sems,
    )
    for copy in copies:
        copy.wait()


def attend_kernel(slots_ref, bias_ref, q_ref, held, out_ref, logs_held):
    rows = out_ref.shape[0] - EXTRA
    logs_held[...] = jnp.zeros_like(logs_held)

    left = lax.broadcasted_iota(jnp.int32, (BLK, LANES), 1) < HEAD_DIM
    key_pos = lax.broadcasted_iota(jnp.int32, (BLK, 4 * BLK), 0)
    query_pos = lax.broadcasted_iota(jnp.int32, (BLK, 4 * BLK), 1) % BLK
    causal = key_pos <= query_pos
    left_row = lax.broadcasted_iota(jnp.int32, (1, LANES), 1) < HEAD_DIM

    def one_block(row, start):
        tiles = q_ref[pl.ds(start, BLK), :].astype(jnp.float32)
        heads = []
        for g in range(4):
            tile = tiles[:, (g // 2) * LANES : (g // 2 + 1) * LANES]
            if g % 2 == 1:
                tile = pltpu.roll(tile, HEAD_DIM, 1)
            heads.append(jnp.where(left, tile, 0.0).astype(jnp.bfloat16))
        stacked = jnp.concatenate(heads, axis=0)
        tops, totals, mixes = [], [], []
        for c in range(0, PICK + 1, CHUNK):
            blocks = [held[slots_ref[row, p]] for p in range(c, c + CHUNK)]
            scores = lax.dot_general(
                jnp.concatenate(blocks, axis=0),
                stacked,
                (((1,), (1,)), ((), ())),
                preferred_element_type=jnp.float32,
            )
            parts = [scores[n * BLK : (n + 1) * BLK] for n in range(CHUNK)]
            if c + CHUNK > PICK:
                parts[-1] = jnp.where(causal, parts[-1], NEGATIVE)
            biases = [bias_ref[row, c + n] for n in range(CHUNK)]
            top = None
            for part, extra in zip(parts, biases):
                own_top = jnp.max(part, axis=0, keepdims=True) + extra
                top = own_top if top is None else jnp.maximum(top, own_top)
            parts = [jnp.exp(part - (top - extra)) for part, extra in zip(parts, biases)]
            exponent = jnp.concatenate(parts, axis=0)
            turned = []
            for n in range(0, CHUNK, 2):
                moved = pltpu.roll(blocks[n].astype(jnp.float32), HEAD_DIM, 1)
                turned.append(
                    jnp.where(left, moved, blocks[n + 1].astype(jnp.float32)).astype(jnp.bfloat16)
                )
            tops.append(top)
            totals.append(jnp.sum(exponent, axis=0, keepdims=True))
            mixes.append(
                jnp.dot(
                    jnp.concatenate(turned, axis=1),
                    exponent.astype(jnp.bfloat16),
                    preferred_element_type=jnp.float32,
                )
            )
        top = functools.reduce(jnp.maximum, tops)
        shares = [jnp.exp(one - top) for one in tops]
        total = functools.reduce(jnp.add, [w * one for w, one in zip(shares, totals)])
        inverse = 1.0 / total
        mixed = functools.reduce(
            jnp.add, [(w * inverse) * one for w, one in zip(shares, mixes)]
        )
        flat = []
        for t in range(2):
            tile = mixed[:, t * LANES : (t + 1) * LANES].T
            flat.append(jnp.concatenate([tile[:HEAD_DIM], tile[HEAD_DIM:]], axis=1))
        return jnp.concatenate(flat, axis=1).astype(jnp.bfloat16), top + jnp.log(total)

    def pair(p, carry):
        logs = []
        for u in range(2):
            start = pl.multiple_of((2 * p + u) * BLK, BLK)
            att, log = one_block(2 * p + u, start)
            out_ref[pl.ds(start, BLK), :] = att
            logs.append(log)
        place = pl.ds(pl.multiple_of(p * LANES, LANES), LANES)
        for t in range(2):
            one = logs[0][:, t * LANES : (t + 1) * LANES]
            two = logs[1][:, t * LANES : (t + 1) * LANES]
            pieces_of = (
                jnp.where(left_row, one, pltpu.roll(two, HEAD_DIM, 1)),
                jnp.where(left_row, pltpu.roll(one, HEAD_DIM, 1), two),
            )
            for j, log in enumerate(pieces_of):
                head = 2 * t + j
                high = rounded(log)
                middle = rounded(log - high)
                low = log - high - middle
                for k, part in enumerate((high, middle, low)):
                    logs_held[4 * k + head : 4 * k + head + 1, place] = part
        return carry

    lax.fori_loop(0, HALF_BLOCKS // 2, pair, 0)
    out_ref[rows:, :] = logs_held[...].astype(jnp.bfloat16)


def lse_kernel(where_ref, *rest):
    pieces, keep_ref, give_ref, held = rest[:4], rest[4], rest[5], rest[6]
    core, chip = where_ref[0], where_ref[1]
    for r in range(CHIPS):
        parts = pieces[r][...].astype(jnp.float32)
        held[lax.rem(chip + r, CHIPS)] = parts[0:4] + parts[4:8] + parts[8:12]
    for j in range(2):
        keep_ref[4 * j : 4 * j + 4, :] = held[2 * core + j]
        give_ref[4 * j : 4 * j + 4, :] = held[2 * (1 - core) + j]


def finish_kernel(where_ref, *rest):
    pieces, w_ref, wp_ref, out_ref, held = rest[:4], rest[4], rest[5], rest[6], rest[7]
    core, chip = where_ref[0], where_ref[1]
    rows, width = held.shape[1:]
    for r in range(CHIPS):
        held[lax.rem(chip + r, CHIPS)] = pieces[r][:rows, :]
    projected = None
    for side, w in enumerate((w_ref, wp_ref)):
        owner = core if side == 0 else 1 - core
        for j in range(2):
            term = jnp.dot(
                held[2 * owner + j],
                w[j * width : (j + 1) * width, :],
                preferred_element_type=jnp.float32,
            )
            projected = term if projected is None else projected + term
    scale = lax.rsqrt(jnp.mean(projected * projected, axis=1, keepdims=True) + EPSILON)
    out_ref[...] = (projected * scale).astype(jnp.bfloat16)


SMEM = pl.BlockSpec(memory_space=pltpu.SMEM)
VMEM = pl.BlockSpec(memory_space=pltpu.VMEM)
ANY = pl.BlockSpec(memory_space=pl.ANY)
HBM = pl.BlockSpec(memory_space=pltpu.HBM)


def grant(mib):
    return pltpu.CompilerParams(vmem_limit_bytes=mib * 2**20)


def assemble(pieces, places, total, before=None):
    moved = sum(p.size * 2 for p in pieces)
    resumed = before is not None
    return pl.pallas_call(
        functools.partial(assemble_kernel, places),
        in_specs=[ANY] * (len(pieces) + resumed),
        out_specs=ANY,
        out_shape=pltpu.VMEM((total, BLK, LANES), jnp.bfloat16),
        scratch_shapes=[pltpu.SemaphoreType.DMA((len(pieces),))],
        input_output_aliases={len(pieces): 0} if resumed else {},
        cost_estimate=pl.CostEstimate(
            flops=moved * 100, bytes_accessed=2 * moved, transcendentals=0
        ),
        compiler_params=grant(8),
        name="assemble",
    )(*pieces, *([before] if resumed else []))


def attend(slots, bias, queries, held):
    rows, width = queries.shape[0] - EXTRA, queries.shape[1]
    return pl.pallas_call(
        attend_kernel,
        in_specs=[SMEM, SMEM, VMEM, VMEM],
        out_specs=VMEM,
        out_shape=pltpu.VMEM((rows + EXTRA, width), jnp.bfloat16),
        scratch_shapes=[pltpu.VMEM((EXTRA, rows), jnp.float32)],
        cost_estimate=pl.CostEstimate(
            flops=32 * rows * width * (PICK + 1) * BLK,
            bytes_accessed=rows * (PICK + 1) * LANES * 2,
            transcendentals=0,
        ),
        compiler_params=grant(16),
        name="attend",
    )(slots, bias, queries, held)


def tied(value, *others):
    return lax.optimization_barrier((value,) + others)[0]


def shards(tokens, w_query, w_key, w_value, w_out, chosen):
    core = lax.axis_index("tp")
    index = lax.axis_index("kv")
    planes = lax.axis_size("kv") // CHIPS
    plane, chip = index // CHIPS, index % CHIPS
    here = jnp.stack([core, chip]).astype(jnp.int32)

    def partner(x):
        return lax.ppermute(x, "tp", [(0, 1), (1, 0)])

    def along_y(x, r):
        return lax.ppermute(
            x,
            "kv",
            [
                (z * CHIPS + y, z * CHIPS + (y + r) % CHIPS)
                for z in range(planes)
                for y in range(CHIPS)
            ],
        )

    def hop(x):
        pairs = []
        for z in range(planes):
            for y in range(CHIPS):
                for c, step in enumerate((1, -1)):
                    to = (z + step) % planes
                    pairs.append(((z * CHIPS + y) * 2 + c, (to * CHIPS + y) * 2 + c))
        return lax.ppermute(x, ("kv", "tp"), pairs)

    own = tokens[0]
    rows = own.shape[0]
    wk_peer, wv_peer = partner(w_key), partner(w_value)
    wq_peer = partner(tied(w_query, wk_peer, wv_peer))
    wo_peer = partner(tied(w_out, wk_peer, wv_peer))

    base = index * 2 * rows + core * rows
    cosine, sine = rotary_tables(base + jnp.arange(rows, dtype=jnp.int32))

    width = own.shape[1]
    piece_shape = (HALF_BLOCKS, BLK, LANES)
    kv_out = pl.pallas_call(
        kv_kernel,
        in_specs=[SMEM] + [HBM] * 3 + [VMEM] * 4,
        out_specs=[VMEM] * CHIPS,
        out_shape=[pltpu.VMEM(piece_shape, jnp.bfloat16)] * CHIPS,
        scratch_shapes=[
            pltpu.VMEM((rows, width), jnp.bfloat16),
            pltpu.VMEM(w_key.shape, jnp.bfloat16),
            pltpu.VMEM(w_value.shape, jnp.bfloat16),
            pltpu.VMEM((CHIPS,) + piece_shape, jnp.bfloat16),
            pltpu.SemaphoreType.DMA((3,)),
        ],
        compiler_params=grant(8),
        name="project_kv",
    )(here, own, w_key, w_value, wk_peer, wv_peer, cosine, sine)
    kv_in = [kv_out[0]] + [along_y(kv_out[r], r) for r in range(1, CHIPS)]

    q_shape = (rows + EXTRA, 4 * HEAD_DIM)
    q_out = pl.pallas_call(
        q_kernel,
        in_specs=[SMEM] + [HBM] * 2 + [VMEM] * 4,
        out_specs=[VMEM] * CHIPS,
        out_shape=[pltpu.VMEM(q_shape, jnp.bfloat16)] * CHIPS,
        scratch_shapes=[
            pltpu.VMEM((rows, width), jnp.bfloat16),
            pltpu.VMEM(w_query.shape, jnp.bfloat16),
            pltpu.VMEM((CHIPS, rows, 4 * HEAD_DIM), jnp.bfloat16),
            pltpu.SemaphoreType.DMA((2,)),
        ],
        compiler_params=grant(10),
        name="project_q",
    )(
        here,
        own,
        w_query,
        wq_peer,
        tied(cosine, kv_out[0]),
        sine,
        jnp.pad(chosen[0], ((0, 0), (0, LANES - PICK))),
    )
    chunk = CHIPS * HALF_BLOCKS
    mine = jnp.concatenate(kv_in, axis=0)
    both = jnp.concatenate([mine, partner(mine)], axis=0)

    last = planes // 2
    ring, swapped = {0: both}, {}
    q_in = [q_out[0]]
    for n in range(1, last + 1):
        moving = ring[n - 1]
        if n == 2:
            moving, *q_ready = lax.optimization_barrier((moving,) + tuple(q_out))
            q_in = [q_ready[0]] + [along_y(q_ready[r], r) for r in range(1, CHIPS)]
            swapped[1] = partner(moving)
        if n == 3:
            swapped[2] = partner(moving)
            moving, swapped[1] = lax.optimization_barrier((moving, swapped[1]))
        if n == last and n > 2:
            moving, swapped[n - 2], *q_in = lax.optimization_barrier(
                (moving, swapped[n - 2]) + tuple(q_in)
            )
        ring[n] = hop(moving if n < last else moving[:chunk])
    if last < 2:
        q_in = [q_out[0]] + [along_y(q_out[r], r) for r in range(1, CHIPS)]
    for n in range(1, last):
        if n not in swapped:
            swapped[n] = partner(ring[n])

    total = 2 * planes * chunk
    early = [(ring[n], 2 * n * chunk) for n in range(last)]
    early += [(swapped[n], 2 * (planes - n) * chunk) for n in range(1, last)]
    held = assemble([p for p, _ in early], [at for _, at in early], total)
    late = [ring[last], partner(ring[last])]
    held = assemble(late, [2 * last * chunk, (2 * last + 1) * chunk], total, held)

    picks = jnp.stack([q[rows : rows + HALF_BLOCKS, :PICK] for q in q_in]).astype(jnp.int32)
    shift = jnp.arange(CHIPS, dtype=jnp.int32)
    source = (chip - shift) % CHIPS
    own_block = (
        plane * (8 * CHIPS)
        + source[:, None] * 8
        + core * HALF_BLOCKS
        + jnp.arange(HALF_BLOCKS, dtype=jnp.int32)[None, :]
    )
    blocks = jnp.concatenate([picks, own_block[:, :, None]], axis=2)
    bias = jnp.where(blocks >= 0, 0.0, NEGATIVE).astype(jnp.float32)
    blocks = jnp.maximum(blocks, 0)
    half = blocks // HALF_BLOCKS % 2
    distance = (plane - blocks // (8 * CHIPS)) % planes
    turn = (chip - blocks // 8 % CHIPS) % CHIPS
    place = jnp.where(core == 0, distance, (planes - distance) % planes)
    half = jnp.where(
        distance % last == 0, half ^ core, jnp.where(distance < last, half, 1 - half)
    )
    slots = ((place * 2 + half) * CHIPS + turn) * HALF_BLOCKS + blocks % HALF_BLOCKS

    att = {}
    for r in (2, 1, 3, 0):
        done = attend(slots[r], bias[r], q_in[r], held)
        att[r] = along_y(done, -r) if r else done

    tail = rows // EXTRA
    keep, give = pl.pallas_call(
        lse_kernel,
        grid=(1,),
        in_specs=[SMEM] + [pl.BlockSpec((EXTRA, rows), lambda i: (tail, 0))] * CHIPS,
        out_specs=[pl.BlockSpec((8, rows), lambda i: (0, 0))] * 2,
        out_shape=[jax.ShapeDtypeStruct((8, rows), jnp.float32)] * 2,
        scratch_shapes=[pltpu.VMEM((CHIPS, 4, rows), jnp.float32)],
        compiler_params=grant(4),
        name="sort_logsums",
    )(here, *[att[r] for r in range(CHIPS)])
    got = partner(give)
    normed = pl.pallas_call(
        finish_kernel,
        in_specs=[SMEM] + [VMEM] * (CHIPS + 2),
        out_specs=VMEM,
        out_shape=jax.ShapeDtypeStruct((rows, w_out.shape[1]), jnp.bfloat16),
        scratch_shapes=[pltpu.VMEM((CHIPS, rows, 4 * HEAD_DIM), jnp.bfloat16)],
        compiler_params=grant(10),
        name="finish",
    )(here, *[att[r] for r in range(CHIPS)], w_out, wo_peer)
    first = jnp.where(core == 0, keep, got)
    second = jnp.where(core == 0, got, keep)
    logsums = jnp.concatenate([first, second], axis=1).T
    return (normed[None], logsums[None])


def solution(mesh):
    placed = (
        P("dp", ("kv", "tp"), None),
        P(None, "tp"),
        P(None, "tp"),
        P(None, "tp"),
        P("tp", None),
        P("dp", "kv", None),
    )
    return jax.shard_map(
        shards,
        mesh=mesh,
        in_specs=placed,
        out_specs=(P("dp", ("kv", "tp"), None), P("dp", "kv", "tp")),
        check_vma=False,
    )
```

```python
import functools

import jax
import jax.numpy as jnp
from jax import lax
from jax.experimental import pallas as pl
from jax.experimental.pallas import tpu as pltpu
from jax.sharding import PartitionSpec as P

HEAD_DIM = 64
BLK = 64
PICK = 15
THETA_BASE = 10000.0
NEGATIVE = -1e30
EPSILON = 1e-06
LANES = 128
CHIPS = 4
HALF_BLOCKS = 4
CHUNK = 16
EXTRA = 16


def rotary_tables(positions):
    half = HEAD_DIM // 2
    inverse = THETA_BASE ** (-jnp.arange(half, dtype=jnp.float32) / half)
    angles = positions.astype(jnp.float32)[:, None] * inverse[None, :]
    cosine = jnp.cos(angles)
    sine = jnp.sin(angles)
    return (
        jnp.concatenate([cosine] * 4, axis=1),
        jnp.concatenate([-sine, sine, -sine, sine], axis=1),
    )


def rotated(values, cosine, sine):
    lane = lax.broadcasted_iota(jnp.int32, values.shape, 1)
    ahead = pltpu.roll(values, LANES - HEAD_DIM // 2, 1)
    behind = pltpu.roll(values, HEAD_DIM // 2, 1)
    swapped = jnp.where(lane % HEAD_DIM < HEAD_DIM // 2, ahead, behind)
    return values * cosine + swapped * sine


def rounded(x):
    return x.astype(jnp.bfloat16).astype(jnp.float32)


def fetch_all(pairs, sems):
    copies = [
        pltpu.make_async_copy(src, dst, sems.at[n]) for n, (src, dst) in enumerate(pairs)
    ]
    for copy in copies:
        copy.start()
    return copies


def kv_kernel(where_ref, x_hbm, wk_hbm, wv_hbm, wkp_ref, wvp_ref, cos_ref, sin_ref, *rest):
    outs, (x_ref, wk_ref, wv_ref, held, sems) = rest[:CHIPS], rest[CHIPS:]
    copies = fetch_all([(x_hbm, x_ref), (wk_hbm, wk_ref), (wv_hbm, wv_ref)], sems)
    core, chip = where_ref[0], where_ref[1]
    for copy in copies:
        copy.wait()
    piece = x_ref[...]
    for side, (wk, wv) in enumerate(((wk_ref, wv_ref), (wkp_ref, wvp_ref))):
        owner = core if side == 0 else 1 - core
        keys = rounded(jnp.dot(piece, wk[...], preferred_element_type=jnp.float32))
        keys = rotated(keys, cos_ref[...], sin_ref[...])
        values = jnp.dot(piece, wv[...], preferred_element_type=jnp.float32)
        for b in range(HALF_BLOCKS):
            rows = slice(b * BLK, (b + 1) * BLK)
            turned = values[rows].T
            for j in range(2):
                cols = slice(j * HEAD_DIM, (j + 1) * HEAD_DIM)
                held[2 * owner + j, b] = jnp.concatenate(
                    [keys[rows, cols], turned[cols]], axis=1
                ).astype(jnp.bfloat16)
    for r in range(CHIPS):
        outs[r][...] = held[lax.rem(chip + r, CHIPS)]


def q_kernel(where_ref, x_hbm, wq_hbm, wqp_ref, cos_ref, sin_ref, picks_ref, *rest):
    outs, (x_ref, wq_ref, held, sems) = rest[:CHIPS], rest[CHIPS:]
    copies = fetch_all([(x_hbm, x_ref), (wq_hbm, wq_ref)], sems)
    core, chip = where_ref[0], where_ref[1]
    rows = x_ref.shape[0]
    for copy in copies:
        copy.wait()
    piece = x_ref[...]
    for side, wq in enumerate((wq_ref, wqp_ref)):
        owner = core if side == 0 else 1 - core
        for j in range(2):
            for t in range(2):
                cols = slice((2 * j + t) * LANES, (2 * j + t + 1) * LANES)
                tile = rounded(jnp.dot(piece, wq[:, cols], preferred_element_type=jnp.float32))
                tile = rotated(tile, cos_ref[...], sin_ref[...]).astype(jnp.bfloat16)
                held[2 * owner + j, :, t * LANES : (t + 1) * LANES] = tile * jnp.bfloat16(
                    HEAD_DIM**-0.5
                )
    mine = jnp.where(core == 0, picks_ref[:HALF_BLOCKS, :], picks_ref[HALF_BLOCKS:, :])
    mine = jnp.concatenate(
        [mine.astype(jnp.float32), jnp.zeros((EXTRA - HALF_BLOCKS, LANES), jnp.float32)], axis=0
    ).astype(jnp.bfloat16)
    for r in range(CHIPS):
        outs[r][:rows, :] = held[lax.rem(chip + r, CHIPS)]
        outs[r][rows:, :LANES] = mine
        outs[r][rows:, LANES:] = jnp.zeros_like(mine)


def assemble_kernel(places, *refs):
    pieces = refs[: len(places)]
    out_ref, sems = refs[-2:]
    copies = fetch_all(
        [
            (piece, out_ref.at[pl.ds(place, piece.shape[0])])
            for piece, place in zip(pieces, places)
        ],
        sems,
    )
    for copy in copies:
        copy.wait()


def attend_kernel(slots_ref, bias_ref, q_ref, held, out_ref, logs_held):
    rows = out_ref.shape[0] - EXTRA
    logs_held[...] = jnp.zeros_like(logs_held)

    left = lax.broadcasted_iota(jnp.int32, (BLK, LANES), 1) < HEAD_DIM
    key_pos = lax.broadcasted_iota(jnp.int32, (BLK, 4 * BLK), 0)
    query_pos = lax.broadcasted_iota(jnp.int32, (BLK, 4 * BLK), 1) % BLK
    causal = key_pos <= query_pos
    left_row = lax.broadcasted_iota(jnp.int32, (1, LANES), 1) < HEAD_DIM

    def one_block(row, start):
        tiles = q_ref[pl.ds(start, BLK), :].astype(jnp.float32)
        heads = []
        for g in range(4):
            tile = tiles[:, (g // 2) * LANES : (g // 2 + 1) * LANES]
            if g % 2 == 1:
                tile = pltpu.roll(tile, HEAD_DIM, 1)
            heads.append(jnp.where(left, tile, 0.0).astype(jnp.bfloat16))
        stacked = jnp.concatenate(heads, axis=0)
        tops, totals, mixes = [], [], []
        for c in range(0, PICK + 1, CHUNK):
            blocks = [held[slots_ref[row, p]] for p in range(c, c + CHUNK)]
            scores = lax.dot_general(
                jnp.concatenate(blocks, axis=0),
                stacked,
                (((1,), (1,)), ((), ())),
                preferred_element_type=jnp.float32,
            )
            parts = [scores[n * BLK : (n + 1) * BLK] for n in range(CHUNK)]
            if c + CHUNK > PICK:
                parts[-1] = jnp.where(causal, parts[-1], NEGATIVE)
            biases = [bias_ref[row, c + n] for n in range(CHUNK)]
            top = None
            for part, extra in zip(parts, biases):
                own_top = jnp.max(part, axis=0, keepdims=True) + extra
                top = own_top if top is None else jnp.maximum(top, own_top)
            parts = [jnp.exp(part - (top - extra)) for part, extra in zip(parts, biases)]
            exponent = jnp.concatenate(parts, axis=0)
            turned = []
            for n in range(0, CHUNK, 2):
                moved = pltpu.roll(blocks[n], HEAD_DIM, 1)
                turned.append(jnp.where(left, moved, blocks[n + 1]))
            tops.append(top)
            totals.append(jnp.sum(exponent, axis=0, keepdims=True))
            mixes.append(
                jnp.dot(
                    jnp.concatenate(turned, axis=1),
                    exponent.astype(jnp.bfloat16),
                    preferred_element_type=jnp.float32,
                )
            )
        top = functools.reduce(jnp.maximum, tops)
        shares = [jnp.exp(one - top) for one in tops]
        total = functools.reduce(jnp.add, [w * one for w, one in zip(shares, totals)])
        inverse = 1.0 / total
        mixed = functools.reduce(
            jnp.add, [(w * inverse) * one for w, one in zip(shares, mixes)]
        )
        flat = []
        for t in range(2):
            tile = mixed[:, t * LANES : (t + 1) * LANES].T
            flat.append(jnp.concatenate([tile[:HEAD_DIM], tile[HEAD_DIM:]], axis=1))
        return jnp.concatenate(flat, axis=1).astype(jnp.bfloat16), top + jnp.log(total)

    def pair(p, carry):
        logs = []
        for u in range(2):
            start = pl.multiple_of((2 * p + u) * BLK, BLK)
            att, log = one_block(2 * p + u, start)
            out_ref[pl.ds(start, BLK), :] = att
            logs.append(log)
        place = pl.ds(pl.multiple_of(p * LANES, LANES), LANES)
        for t in range(2):
            one = logs[0][:, t * LANES : (t + 1) * LANES]
            two = logs[1][:, t * LANES : (t + 1) * LANES]
            pieces_of = (
                jnp.where(left_row, one, pltpu.roll(two, HEAD_DIM, 1)),
                jnp.where(left_row, pltpu.roll(one, HEAD_DIM, 1), two),
            )
            for j, log in enumerate(pieces_of):
                head = 2 * t + j
                high = rounded(log)
                middle = rounded(log - high)
                low = log - high - middle
                for k, part in enumerate((high, middle, low)):
                    logs_held[4 * k + head : 4 * k + head + 1, place] = part
        return carry

    lax.fori_loop(0, HALF_BLOCKS // 2, pair, 0)
    out_ref[rows:, :] = logs_held[...].astype(jnp.bfloat16)


def lse_kernel(where_ref, *rest):
    pieces, keep_ref, give_ref, held = rest[:4], rest[4], rest[5], rest[6]
    core, chip = where_ref[0], where_ref[1]
    for r in range(CHIPS):
        parts = pieces[r][...].astype(jnp.float32)
        held[lax.rem(chip + r, CHIPS)] = parts[0:4] + parts[4:8] + parts[8:12]
    for j in range(2):
        keep_ref[4 * j : 4 * j + 4, :] = held[2 * core + j]
        give_ref[4 * j : 4 * j + 4, :] = held[2 * (1 - core) + j]


def finish_kernel(where_ref, *rest):
    pieces, w_ref, wp_ref, out_ref, held = rest[:4], rest[4], rest[5], rest[6], rest[7]
    core, chip = where_ref[0], where_ref[1]
    rows, width = held.shape[1:]
    for r in range(CHIPS):
        held[lax.rem(chip + r, CHIPS)] = pieces[r][:rows, :]
    projected = None
    for side, w in enumerate((w_ref, wp_ref)):
        owner = core if side == 0 else 1 - core
        for j in range(2):
            term = jnp.dot(
                held[2 * owner + j],
                w[j * width : (j + 1) * width, :],
                preferred_element_type=jnp.float32,
            )
            projected = term if projected is None else projected + term
    scale = lax.rsqrt(jnp.mean(projected * projected, axis=1, keepdims=True) + EPSILON)
    out_ref[...] = (projected * scale).astype(jnp.bfloat16)


SMEM = pl.BlockSpec(memory_space=pltpu.SMEM)
VMEM = pl.BlockSpec(memory_space=pltpu.VMEM)
ANY = pl.BlockSpec(memory_space=pl.ANY)
HBM = pl.BlockSpec(memory_space=pltpu.HBM)


def grant(mib):
    return pltpu.CompilerParams(vmem_limit_bytes=mib * 2**20)


def assemble(pieces, places, total, before=None):
    moved = sum(p.size * 2 for p in pieces)
    resumed = before is not None
    return pl.pallas_call(
        functools.partial(assemble_kernel, places),
        in_specs=[ANY] * (len(pieces) + resumed),
        out_specs=ANY,
        out_shape=pltpu.VMEM((total, BLK, LANES), jnp.bfloat16),
        scratch_shapes=[pltpu.SemaphoreType.DMA((len(pieces),))],
        input_output_aliases={len(pieces): 0} if resumed else {},
        cost_estimate=pl.CostEstimate(
            flops=moved * 100, bytes_accessed=2 * moved, transcendentals=0
        ),
        compiler_params=grant(8),
        name="assemble",
    )(*pieces, *([before] if resumed else []))


def attend(slots, bias, queries, held):
    rows, width = queries.shape[0] - EXTRA, queries.shape[1]
    return pl.pallas_call(
        attend_kernel,
        in_specs=[SMEM, SMEM, VMEM, VMEM],
        out_specs=VMEM,
        out_shape=pltpu.VMEM((rows + EXTRA, width), jnp.bfloat16),
        scratch_shapes=[pltpu.VMEM((EXTRA, rows), jnp.float32)],
        cost_estimate=pl.CostEstimate(
            flops=32 * rows * width * (PICK + 1) * BLK,
            bytes_accessed=rows * (PICK + 1) * LANES * 2,
            transcendentals=0,
        ),
        compiler_params=grant(16),
        name="attend",
    )(slots, bias, queries, held)


def tied(value, *others):
    return lax.optimization_barrier((value,) + others)[0]


def shards(tokens, w_query, w_key, w_value, w_out, chosen):
    core = lax.axis_index("tp")
    index = lax.axis_index("kv")
    planes = lax.axis_size("kv") // CHIPS
    plane, chip = index // CHIPS, index % CHIPS
    here = jnp.stack([core, chip]).astype(jnp.int32)

    def partner(x):
        return lax.ppermute(x, "tp", [(0, 1), (1, 0)])

    def along_y(x, r):
        return lax.ppermute(
            x,
            "kv",
            [
                (z * CHIPS + y, z * CHIPS + (y + r) % CHIPS)
                for z in range(planes)
                for y in range(CHIPS)
            ],
        )

    def hop(x):
        pairs = []
        for z in range(planes):
            for y in range(CHIPS):
                for c, step in enumerate((1, -1)):
                    to = (z + step) % planes
                    pairs.append(((z * CHIPS + y) * 2 + c, (to * CHIPS + y) * 2 + c))
        return lax.ppermute(x, ("kv", "tp"), pairs)

    own = tokens[0]
    rows = own.shape[0]
    wk_peer, wv_peer = partner(w_key), partner(w_value)
    wq_peer = partner(tied(w_query, wk_peer, wv_peer))
    wo_peer = partner(tied(w_out, wk_peer, wv_peer))

    base = index * 2 * rows + core * rows
    cosine, sine = rotary_tables(base + jnp.arange(rows, dtype=jnp.int32))

    width = own.shape[1]
    piece_shape = (HALF_BLOCKS, BLK, LANES)
    kv_out = pl.pallas_call(
        kv_kernel,
        in_specs=[SMEM] + [HBM] * 3 + [VMEM] * 4,
        out_specs=[VMEM] * CHIPS,
        out_shape=[pltpu.VMEM(piece_shape, jnp.bfloat16)] * CHIPS,
        scratch_shapes=[
            pltpu.VMEM((rows, width), jnp.bfloat16),
            pltpu.VMEM(w_key.shape, jnp.bfloat16),
            pltpu.VMEM(w_value.shape, jnp.bfloat16),
            pltpu.VMEM((CHIPS,) + piece_shape, jnp.bfloat16),
            pltpu.SemaphoreType.DMA((3,)),
        ],
        compiler_params=grant(58),
        name="project_kv",
    )(here, own, w_key, w_value, wk_peer, wv_peer, cosine, sine)
    kv_in = [kv_out[0]] + [along_y(kv_out[r], r) for r in range(1, CHIPS)]

    q_shape = (rows + EXTRA, 4 * HEAD_DIM)
    q_out = pl.pallas_call(
        q_kernel,
        in_specs=[SMEM] + [HBM] * 2 + [VMEM] * 4,
        out_specs=[VMEM] * CHIPS,
        out_shape=[pltpu.VMEM(q_shape, jnp.bfloat16)] * CHIPS,
        scratch_shapes=[
            pltpu.VMEM((rows, width), jnp.bfloat16),
            pltpu.VMEM(w_query.shape, jnp.bfloat16),
            pltpu.VMEM((CHIPS, rows, 4 * HEAD_DIM), jnp.bfloat16),
            pltpu.SemaphoreType.DMA((2,)),
        ],
        compiler_params=grant(10),
        name="project_q",
    )(
        here,
        own,
        w_query,
        wq_peer,
        tied(cosine, kv_out[0]),
        sine,
        jnp.pad(chosen[0], ((0, 0), (0, LANES - PICK))),
    )
    chunk = CHIPS * HALF_BLOCKS
    mine = jnp.concatenate(kv_in, axis=0)
    both = jnp.concatenate([mine, partner(mine)], axis=0)

    last = planes // 2
    ring, swapped = {0: both}, {}
    q_in = [q_out[0]]
    for n in range(1, last + 1):
        moving = ring[n - 1]
        if n == 2:
            moving, *q_ready = lax.optimization_barrier((moving,) + tuple(q_out))
            q_in = [q_ready[0]] + [along_y(q_ready[r], r) for r in range(1, CHIPS)]
            swapped[1] = partner(moving)
        if n == 3:
            swapped[2] = partner(moving)
            moving, swapped[1], *q_in = lax.optimization_barrier(
                (moving, swapped[1]) + tuple(q_in)
            )
        ring[n] = hop(moving if n < last else moving[:chunk])
    if last < 2:
        q_in = [q_out[0]] + [along_y(q_out[r], r) for r in range(1, CHIPS)]
    for n in range(1, last):
        if n not in swapped:
            swapped[n] = partner(ring[n])

    total = 2 * planes * chunk
    early = [(ring[n], 2 * n * chunk) for n in range(last)]
    early += [(swapped[n], 2 * (planes - n) * chunk) for n in range(1, last)]
    held = assemble([p for p, _ in early], [at for _, at in early], total)
    late = [ring[last], partner(ring[last])]
    held = assemble(late, [2 * last * chunk, (2 * last + 1) * chunk], total, held)

    picks = jnp.stack([q[rows : rows + HALF_BLOCKS, :PICK] for q in q_in]).astype(jnp.int32)
    shift = jnp.arange(CHIPS, dtype=jnp.int32)
    source = (chip - shift) % CHIPS
    own_block = (
        plane * (8 * CHIPS)
        + source[:, None] * 8
        + core * HALF_BLOCKS
        + jnp.arange(HALF_BLOCKS, dtype=jnp.int32)[None, :]
    )
    blocks = jnp.concatenate([picks, own_block[:, :, None]], axis=2)
    bias = jnp.where(blocks >= 0, 0.0, NEGATIVE).astype(jnp.float32)
    blocks = jnp.maximum(blocks, 0)
    half = blocks // HALF_BLOCKS % 2
    distance = (plane - blocks // (8 * CHIPS)) % planes
    turn = (chip - blocks // 8 % CHIPS) % CHIPS
    place = jnp.where(core == 0, distance, (planes - distance) % planes)
    half = jnp.where(
        distance % last == 0, half ^ core, jnp.where(distance < last, half, 1 - half)
    )
    slots = ((place * 2 + half) * CHIPS + turn) * HALF_BLOCKS + blocks % HALF_BLOCKS

    att = {}
    for r in (2, 1, 3, 0):
        done = attend(slots[r], bias[r], q_in[r], held)
        att[r] = along_y(done, -r) if r else done

    tail = rows // EXTRA
    keep, give = pl.pallas_call(
        lse_kernel,
        grid=(1,),
        in_specs=[SMEM] + [pl.BlockSpec((EXTRA, rows), lambda i: (tail, 0))] * CHIPS,
        out_specs=[pl.BlockSpec((8, rows), lambda i: (0, 0))] * 2,
        out_shape=[jax.ShapeDtypeStruct((8, rows), jnp.float32)] * 2,
        scratch_shapes=[pltpu.VMEM((CHIPS, 4, rows), jnp.float32)],
        compiler_params=grant(4),
        name="sort_logsums",
    )(here, *[att[r] for r in range(CHIPS)])
    got = partner(give)
    normed = pl.pallas_call(
        finish_kernel,
        in_specs=[SMEM] + [VMEM] * (CHIPS + 2),
        out_specs=VMEM,
        out_shape=jax.ShapeDtypeStruct((rows, w_out.shape[1]), jnp.bfloat16),
        scratch_shapes=[pltpu.VMEM((CHIPS, rows, 4 * HEAD_DIM), jnp.bfloat16)],
        compiler_params=grant(10),
        name="finish",
    )(here, *[att[r] for r in range(CHIPS)], w_out, wo_peer)
    first = jnp.where(core == 0, keep, got)
    second = jnp.where(core == 0, got, keep)
    logsums = jnp.concatenate([first, second], axis=1).T
    return (normed[None], logsums[None])


def solution(mesh):
    placed = (
        P("dp", ("kv", "tp"), None),
        P(None, "tp"),
        P(None, "tp"),
        P(None, "tp"),
        P("tp", None),
        P("dp", "kv", None),
    )
    return jax.shard_map(
        shards,
        mesh=mesh,
        in_specs=placed,
        out_specs=(P("dp", ("kv", "tp"), None), P("dp", "kv", "tp")),
        check_vma=False,
    )
```

```python
import functools

import jax
import jax.numpy as jnp
from jax import lax
from jax.experimental import pallas as pl
from jax.experimental.pallas import tpu as pltpu
from jax.sharding import PartitionSpec as P

HEAD_DIM = 64
BLK = 64
PICK = 15
THETA_BASE = 10000.0
NEGATIVE = -1e30
EPSILON = 1e-06
LANES = 128
CHIPS = 4
HALF_BLOCKS = 4
CHUNK = 16
EXTRA = 16


def rotary_tables(positions):
    half = HEAD_DIM // 2
    inverse = THETA_BASE ** (-jnp.arange(half, dtype=jnp.float32) / half)
    angles = positions.astype(jnp.float32)[:, None] * inverse[None, :]
    cosine = jnp.cos(angles)
    sine = jnp.sin(angles)
    return (
        jnp.concatenate([cosine] * 4, axis=1),
        jnp.concatenate([-sine, sine, -sine, sine], axis=1),
    )


def rotated(values, cosine, sine):
    lane = lax.broadcasted_iota(jnp.int32, values.shape, 1)
    ahead = pltpu.roll(values, LANES - HEAD_DIM // 2, 1)
    behind = pltpu.roll(values, HEAD_DIM // 2, 1)
    swapped = jnp.where(lane % HEAD_DIM < HEAD_DIM // 2, ahead, behind)
    return values * cosine + swapped * sine


def rounded(x):
    return x.astype(jnp.bfloat16).astype(jnp.float32)


def fetch_all(pairs, sems):
    copies = [
        pltpu.make_async_copy(src, dst, sems.at[n]) for n, (src, dst) in enumerate(pairs)
    ]
    for copy in copies:
        copy.start()
    return copies


def kv_kernel(where_ref, x_hbm, wk_hbm, wv_hbm, wkp_ref, wvp_ref, cos_ref, sin_ref, *rest):
    outs, (x_ref, wk_ref, wv_ref, held, sems) = rest[:CHIPS], rest[CHIPS:]
    copies = fetch_all([(x_hbm, x_ref), (wk_hbm, wk_ref), (wv_hbm, wv_ref)], sems)
    core, chip = where_ref[0], where_ref[1]
    for copy in copies:
        copy.wait()
    piece = x_ref[...]
    for side, (wk, wv) in enumerate(((wk_ref, wv_ref), (wkp_ref, wvp_ref))):
        owner = core if side == 0 else 1 - core
        keys = rounded(jnp.dot(piece, wk[...], preferred_element_type=jnp.float32))
        keys = rotated(keys, cos_ref[...], sin_ref[...])
        values = jnp.dot(piece, wv[...], preferred_element_type=jnp.float32)
        for b in range(HALF_BLOCKS):
            rows = slice(b * BLK, (b + 1) * BLK)
            turned = values[rows].T
            for j in range(2):
                cols = slice(j * HEAD_DIM, (j + 1) * HEAD_DIM)
                held[2 * owner + j, b] = jnp.concatenate(
                    [keys[rows, cols], turned[cols]], axis=1
                ).astype(jnp.bfloat16)
    for r in range(CHIPS):
        outs[r][...] = held[lax.rem(chip + r, CHIPS)]


def q_kernel(where_ref, x_hbm, wq_hbm, wqp_ref, cos_ref, sin_ref, picks_ref, *rest):
    outs, (x_ref, wq_ref, held, sems) = rest[:CHIPS], rest[CHIPS:]
    copies = fetch_all([(x_hbm, x_ref), (wq_hbm, wq_ref)], sems)
    core, chip = where_ref[0], where_ref[1]
    rows = x_ref.shape[0]
    for copy in copies:
        copy.wait()
    piece = x_ref[...]
    for side, wq in enumerate((wq_ref, wqp_ref)):
        owner = core if side == 0 else 1 - core
        for j in range(2):
            for t in range(2):
                cols = slice((2 * j + t) * LANES, (2 * j + t + 1) * LANES)
                tile = rounded(jnp.dot(piece, wq[:, cols], preferred_element_type=jnp.float32))
                tile = rotated(tile, cos_ref[...], sin_ref[...]).astype(jnp.bfloat16)
                held[2 * owner + j, :, t * LANES : (t + 1) * LANES] = tile * jnp.bfloat16(
                    HEAD_DIM**-0.5
                )
    mine = jnp.where(core == 0, picks_ref[:HALF_BLOCKS, :], picks_ref[HALF_BLOCKS:, :])
    mine = jnp.concatenate(
        [mine.astype(jnp.float32), jnp.zeros((EXTRA - HALF_BLOCKS, LANES), jnp.float32)], axis=0
    ).astype(jnp.bfloat16)
    for r in range(CHIPS):
        outs[r][:rows, :] = held[lax.rem(chip + r, CHIPS)]
        outs[r][rows:, :LANES] = mine
        outs[r][rows:, LANES:] = jnp.zeros_like(mine)


def assemble_kernel(places, *refs):
    pieces = refs[: len(places)]
    out_ref, sems = refs[-2:]
    copies = fetch_all(
        [
            (piece, out_ref.at[pl.ds(place, piece.shape[0])])
            for piece, place in zip(pieces, places)
        ],
        sems,
    )
    for copy in copies:
        copy.wait()


def attend_kernel(slots_ref, bias_ref, q_ref, held, out_ref, logs_held):
    rows = out_ref.shape[0] - EXTRA
    logs_held[...] = jnp.zeros_like(logs_held)

    left = lax.broadcasted_iota(jnp.int32, (BLK, LANES), 1) < HEAD_DIM
    key_pos = lax.broadcasted_iota(jnp.int32, (BLK, 4 * BLK), 0)
    query_pos = lax.broadcasted_iota(jnp.int32, (BLK, 4 * BLK), 1) % BLK
    causal = key_pos <= query_pos
    left_row = lax.broadcasted_iota(jnp.int32, (1, LANES), 1) < HEAD_DIM

    def one_block(row, start):
        tiles = q_ref[pl.ds(start, BLK), :].astype(jnp.float32)
        heads = []
        for g in range(4):
            tile = tiles[:, (g // 2) * LANES : (g // 2 + 1) * LANES]
            if g % 2 == 1:
                tile = pltpu.roll(tile, HEAD_DIM, 1)
            heads.append(jnp.where(left, tile, 0.0).astype(jnp.bfloat16))
        stacked = jnp.concatenate(heads, axis=0)
        tops, totals, mixes = [], [], []
        for c in range(0, PICK + 1, CHUNK):
            blocks = [held[slots_ref[row, p]] for p in range(c, c + CHUNK)]
            scores = lax.dot_general(
                jnp.concatenate(blocks, axis=0),
                stacked,
                (((1,), (1,)), ((), ())),
                preferred_element_type=jnp.float32,
            )
            parts = [scores[n * BLK : (n + 1) * BLK] for n in range(CHUNK)]
            if c + CHUNK > PICK:
                parts[-1] = jnp.where(causal, parts[-1], NEGATIVE)
            biases = [bias_ref[row, c + n] for n in range(CHUNK)]
            top = None
            for part, extra in zip(parts, biases):
                own_top = jnp.max(part, axis=0, keepdims=True) + extra
                top = own_top if top is None else jnp.maximum(top, own_top)
            parts = [jnp.exp(part - (top - extra)) for part, extra in zip(parts, biases)]
            exponent = jnp.concatenate(parts, axis=0)
            turned = []
            for n in range(0, CHUNK, 2):
                moved = pltpu.roll(blocks[n], HEAD_DIM, 1)
                turned.append(jnp.where(left, moved, blocks[n + 1]))
            tops.append(top)
            totals.append(jnp.sum(exponent, axis=0, keepdims=True))
            mixes.append(
                jnp.dot(
                    jnp.concatenate(turned, axis=1),
                    exponent.astype(jnp.bfloat16),
                    preferred_element_type=jnp.float32,
                )
            )
        top = functools.reduce(jnp.maximum, tops)
        shares = [jnp.exp(one - top) for one in tops]
        total = functools.reduce(jnp.add, [w * one for w, one in zip(shares, totals)])
        inverse = 1.0 / total
        mixed = functools.reduce(
            jnp.add, [(w * inverse) * one for w, one in zip(shares, mixes)]
        )
        flat = []
        for t in range(2):
            tile = mixed[:, t * LANES : (t + 1) * LANES].T
            flat.append(jnp.concatenate([tile[:HEAD_DIM], tile[HEAD_DIM:]], axis=1))
        return jnp.concatenate(flat, axis=1).astype(jnp.bfloat16), top + jnp.log(total)

    def pair(p, carry):
        logs = []
        for u in range(2):
            start = pl.multiple_of((2 * p + u) * BLK, BLK)
            att, log = one_block(2 * p + u, start)
            out_ref[pl.ds(start, BLK), :] = att
            logs.append(log)
        place = pl.ds(pl.multiple_of(p * LANES, LANES), LANES)
        for t in range(2):
            one = logs[0][:, t * LANES : (t + 1) * LANES]
            two = logs[1][:, t * LANES : (t + 1) * LANES]
            pieces_of = (
                jnp.where(left_row, one, pltpu.roll(two, HEAD_DIM, 1)),
                jnp.where(left_row, pltpu.roll(one, HEAD_DIM, 1), two),
            )
            for j, log in enumerate(pieces_of):
                head = 2 * t + j
                high = rounded(log)
                middle = rounded(log - high)
                low = log - high - middle
                for k, part in enumerate((high, middle, low)):
                    logs_held[4 * k + head : 4 * k + head + 1, place] = part
        return carry

    lax.fori_loop(0, HALF_BLOCKS // 2, pair, 0)
    out_ref[rows:, :] = logs_held[...].astype(jnp.bfloat16)


def lse_kernel(where_ref, *rest):
    pieces, keep_ref, give_ref, held = rest[:4], rest[4], rest[5], rest[6]
    core, chip = where_ref[0], where_ref[1]
    for r in range(CHIPS):
        parts = pieces[r][...].astype(jnp.float32)
        held[lax.rem(chip + r, CHIPS)] = parts[0:4] + parts[4:8] + parts[8:12]
    for j in range(2):
        keep_ref[4 * j : 4 * j + 4, :] = held[2 * core + j]
        give_ref[4 * j : 4 * j + 4, :] = held[2 * (1 - core) + j]


def finish_kernel(where_ref, *rest):
    pieces, w_ref, wp_ref, out_ref, held = rest[:4], rest[4], rest[5], rest[6], rest[7]
    core, chip = where_ref[0], where_ref[1]
    rows, width = held.shape[1:]
    for r in range(CHIPS):
        held[lax.rem(chip + r, CHIPS)] = pieces[r][:rows, :]
    projected = None
    for side, w in enumerate((w_ref, wp_ref)):
        owner = core if side == 0 else 1 - core
        for j in range(2):
            term = jnp.dot(
                held[2 * owner + j],
                w[j * width : (j + 1) * width, :],
                preferred_element_type=jnp.float32,
            )
            projected = term if projected is None else projected + term
    scale = lax.rsqrt(jnp.mean(projected * projected, axis=1, keepdims=True) + EPSILON)
    out_ref[...] = (projected * scale).astype(jnp.bfloat16)


SMEM = pl.BlockSpec(memory_space=pltpu.SMEM)
VMEM = pl.BlockSpec(memory_space=pltpu.VMEM)
ANY = pl.BlockSpec(memory_space=pl.ANY)
HBM = pl.BlockSpec(memory_space=pltpu.HBM)


def grant(mib):
    return pltpu.CompilerParams(vmem_limit_bytes=mib * 2**20)


def assemble(pieces, places, total, before=None):
    moved = sum(p.size * 2 for p in pieces)
    resumed = before is not None
    return pl.pallas_call(
        functools.partial(assemble_kernel, places),
        in_specs=[ANY] * (len(pieces) + resumed),
        out_specs=ANY,
        out_shape=pltpu.VMEM((total, BLK, LANES), jnp.bfloat16),
        scratch_shapes=[pltpu.SemaphoreType.DMA((len(pieces),))],
        input_output_aliases={len(pieces): 0} if resumed else {},
        cost_estimate=pl.CostEstimate(
            flops=moved * 100, bytes_accessed=2 * moved, transcendentals=0
        ),
        compiler_params=grant(8),
        name="assemble",
    )(*pieces, *([before] if resumed else []))


def attend(slots, bias, queries, held):
    rows, width = queries.shape[0] - EXTRA, queries.shape[1]
    return pl.pallas_call(
        attend_kernel,
        in_specs=[SMEM, SMEM, VMEM, VMEM],
        out_specs=VMEM,
        out_shape=pltpu.VMEM((rows + EXTRA, width), jnp.bfloat16),
        scratch_shapes=[pltpu.VMEM((EXTRA, rows), jnp.float32)],
        cost_estimate=pl.CostEstimate(
            flops=32 * rows * width * (PICK + 1) * BLK,
            bytes_accessed=rows * (PICK + 1) * LANES * 2,
            transcendentals=0,
        ),
        compiler_params=grant(16),
        name="attend",
    )(slots, bias, queries, held)


def tied(value, *others):
    return lax.optimization_barrier((value,) + others)[0]


def shards(tokens, w_query, w_key, w_value, w_out, chosen):
    core = lax.axis_index("tp")
    index = lax.axis_index("kv")
    planes = lax.axis_size("kv") // CHIPS
    plane, chip = index // CHIPS, index % CHIPS
    here = jnp.stack([core, chip]).astype(jnp.int32)

    def partner(x):
        return lax.ppermute(x, "tp", [(0, 1), (1, 0)])

    def along_y(x, r):
        return lax.ppermute(
            x,
            "kv",
            [
                (z * CHIPS + y, z * CHIPS + (y + r) % CHIPS)
                for z in range(planes)
                for y in range(CHIPS)
            ],
        )

    def hop(x):
        pairs = []
        for z in range(planes):
            for y in range(CHIPS):
                for c, step in enumerate((1, -1)):
                    to = (z + step) % planes
                    pairs.append(((z * CHIPS + y) * 2 + c, (to * CHIPS + y) * 2 + c))
        return lax.ppermute(x, ("kv", "tp"), pairs)

    own = tokens[0]
    rows = own.shape[0]
    wk_peer, wv_peer = partner(w_key), partner(w_value)
    wq_peer = partner(tied(w_query, wk_peer, wv_peer))
    wo_peer = partner(tied(w_out, wk_peer, wv_peer))

    base = index * 2 * rows + core * rows
    cosine, sine = rotary_tables(base + jnp.arange(rows, dtype=jnp.int32))

    width = own.shape[1]
    piece_shape = (HALF_BLOCKS, BLK, LANES)
    kv_out = pl.pallas_call(
        kv_kernel,
        in_specs=[SMEM] + [HBM] * 3 + [VMEM] * 4,
        out_specs=[VMEM] * CHIPS,
        out_shape=[pltpu.VMEM(piece_shape, jnp.bfloat16)] * CHIPS,
        scratch_shapes=[
            pltpu.VMEM((rows, width), jnp.bfloat16),
            pltpu.VMEM(w_key.shape, jnp.bfloat16),
            pltpu.VMEM(w_value.shape, jnp.bfloat16),
            pltpu.VMEM((CHIPS,) + piece_shape, jnp.bfloat16),
            pltpu.SemaphoreType.DMA((3,)),
        ],
        compiler_params=grant(8),
        name="project_kv",
    )(here, own, w_key, w_value, wk_peer, wv_peer, cosine, sine)
    kv_in = [kv_out[0]] + [along_y(kv_out[r], r) for r in range(1, CHIPS)]

    q_shape = (rows + EXTRA, 4 * HEAD_DIM)
    q_out = pl.pallas_call(
        q_kernel,
        in_specs=[SMEM] + [HBM] * 2 + [VMEM] * 4,
        out_specs=[VMEM] * CHIPS,
        out_shape=[pltpu.VMEM(q_shape, jnp.bfloat16)] * CHIPS,
        scratch_shapes=[
            pltpu.VMEM((rows, width), jnp.bfloat16),
            pltpu.VMEM(w_query.shape, jnp.bfloat16),
            pltpu.VMEM((CHIPS, rows, 4 * HEAD_DIM), jnp.bfloat16),
            pltpu.SemaphoreType.DMA((2,)),
        ],
        compiler_params=grant(10),
        name="project_q",
    )(
        here,
        own,
        w_query,
        wq_peer,
        tied(cosine, kv_out[0]),
        sine,
        jnp.pad(chosen[0], ((0, 0), (0, LANES - PICK))),
    )
    chunk = CHIPS * HALF_BLOCKS
    mine = jnp.concatenate(kv_in, axis=0)
    both = jnp.concatenate([mine, partner(mine)], axis=0)

    last = planes // 2
    ring, swapped = {0: both}, {}
    q_in = [q_out[0]]
    for n in range(1, last + 1):
        moving = ring[n - 1]
        if n == 2:
            moving, *q_ready = lax.optimization_barrier((moving,) + tuple(q_out))
            swapped[1] = partner(moving)
        if n == 3:
            swapped[2] = partner(moving)
            moving, swapped[1] = lax.optimization_barrier((moving, swapped[1]))
        if n == last and n > 1:
            ready = [tied(q, moving) for q in q_ready]
            q_in = [ready[0]] + [along_y(ready[r], r) for r in range(1, CHIPS)]
        ring[n] = hop(moving if n < last else moving[:chunk])
    if last < 2:
        q_in = [q_out[0]] + [along_y(q_out[r], r) for r in range(1, CHIPS)]
    for n in range(1, last):
        if n not in swapped:
            swapped[n] = partner(ring[n])

    total = 2 * planes * chunk
    early = [(ring[n], 2 * n * chunk) for n in range(last)]
    early += [(swapped[n], 2 * (planes - n) * chunk) for n in range(1, last)]
    held = assemble([p for p, _ in early], [at for _, at in early], total)
    late = [ring[last], partner(ring[last])]
    held = assemble(late, [2 * last * chunk, (2 * last + 1) * chunk], total, held)

    picks = jnp.stack([q[rows : rows + HALF_BLOCKS, :PICK] for q in q_in]).astype(jnp.int32)
    shift = jnp.arange(CHIPS, dtype=jnp.int32)
    source = (chip - shift) % CHIPS
    own_block = (
        plane * (8 * CHIPS)
        + source[:, None] * 8
        + core * HALF_BLOCKS
        + jnp.arange(HALF_BLOCKS, dtype=jnp.int32)[None, :]
    )
    blocks = jnp.concatenate([picks, own_block[:, :, None]], axis=2)
    bias = jnp.where(blocks >= 0, 0.0, NEGATIVE).astype(jnp.float32)
    blocks = jnp.maximum(blocks, 0)
    half = blocks // HALF_BLOCKS % 2
    distance = (plane - blocks // (8 * CHIPS)) % planes
    turn = (chip - blocks // 8 % CHIPS) % CHIPS
    place = jnp.where(core == 0, distance, (planes - distance) % planes)
    half = jnp.where(
        distance % last == 0, half ^ core, jnp.where(distance < last, half, 1 - half)
    )
    slots = ((place * 2 + half) * CHIPS + turn) * HALF_BLOCKS + blocks % HALF_BLOCKS

    att = {}
    for r in (2, 1, 3, 0):
        done = attend(slots[r], bias[r], q_in[r], held)
        att[r] = along_y(done, -r) if r else done

    tail = rows // EXTRA
    keep, give = pl.pallas_call(
        lse_kernel,
        grid=(1,),
        in_specs=[SMEM] + [pl.BlockSpec((EXTRA, rows), lambda i: (tail, 0))] * CHIPS,
        out_specs=[pl.BlockSpec((8, rows), lambda i: (0, 0))] * 2,
        out_shape=[jax.ShapeDtypeStruct((8, rows), jnp.float32)] * 2,
        scratch_shapes=[pltpu.VMEM((CHIPS, 4, rows), jnp.float32)],
        compiler_params=grant(4),
        name="sort_logsums",
    )(here, *[att[r] for r in range(CHIPS)])
    got = partner(give)
    normed = pl.pallas_call(
        finish_kernel,
        in_specs=[SMEM] + [VMEM] * (CHIPS + 2),
        out_specs=VMEM,
        out_shape=jax.ShapeDtypeStruct((rows, w_out.shape[1]), jnp.bfloat16),
        scratch_shapes=[pltpu.VMEM((CHIPS, rows, 4 * HEAD_DIM), jnp.bfloat16)],
        compiler_params=grant(10),
        name="finish",
    )(here, *[att[r] for r in range(CHIPS)], w_out, wo_peer)
    first = jnp.where(core == 0, keep, got)
    second = jnp.where(core == 0, got, keep)
    logsums = jnp.concatenate([first, second], axis=1).T
    return (normed[None], logsums[None])


def solution(mesh):
    placed = (
        P("dp", ("kv", "tp"), None),
        P(None, "tp"),
        P(None, "tp"),
        P(None, "tp"),
        P("tp", None),
        P("dp", "kv", None),
    )
    return jax.shard_map(
        shards,
        mesh=mesh,
        in_specs=placed,
        out_specs=(P("dp", ("kv", "tp"), None), P("dp", "kv", "tp")),
        check_vma=False,
    )
```

```python
import functools

import jax
import jax.numpy as jnp
from jax import lax
from jax.experimental import pallas as pl
from jax.experimental.pallas import tpu as pltpu
from jax.sharding import PartitionSpec as P

HEAD_DIM = 64
BLK = 64
PICK = 15
THETA_BASE = 10000.0
NEGATIVE = -1e30
EPSILON = 1e-06
LANES = 128
CHIPS = 4
HALF_BLOCKS = 4
CHUNK = 16
EXTRA = 16


def rotary_tables(positions):
    half = HEAD_DIM // 2
    inverse = THETA_BASE ** (-jnp.arange(half, dtype=jnp.float32) / half)
    angles = positions.astype(jnp.float32)[:, None] * inverse[None, :]
    cosine = jnp.cos(angles)
    sine = jnp.sin(angles)
    return (
        jnp.concatenate([cosine] * 4, axis=1),
        jnp.concatenate([-sine, sine, -sine, sine], axis=1),
    )


def rotated(values, cosine, sine):
    lane = lax.broadcasted_iota(jnp.int32, values.shape, 1)
    ahead = pltpu.roll(values, LANES - HEAD_DIM // 2, 1)
    behind = pltpu.roll(values, HEAD_DIM // 2, 1)
    swapped = jnp.where(lane % HEAD_DIM < HEAD_DIM // 2, ahead, behind)
    return values * cosine + swapped * sine


def rounded(x):
    return x.astype(jnp.bfloat16).astype(jnp.float32)


def fetch_all(pairs, sems):
    copies = [
        pltpu.make_async_copy(src, dst, sems.at[n]) for n, (src, dst) in enumerate(pairs)
    ]
    for copy in copies:
        copy.start()
    return copies


def preload_kernel(x, wk, wv, x_out, wk_out, wv_out, sems):
    for copy in fetch_all([(x, x_out), (wk, wk_out), (wv, wv_out)], sems):
        copy.wait()


def kv_kernel(where_ref, x_hbm, wk_hbm, wv_hbm, wkp_ref, wvp_ref, cos_ref, sin_ref, *rest):
    outs, (x_ref, wk_ref, wv_ref, held, sems) = rest[:CHIPS], rest[CHIPS:]
    copies = fetch_all([(x_hbm, x_ref), (wk_hbm, wk_ref), (wv_hbm, wv_ref)], sems)
    core, chip = where_ref[0], where_ref[1]
    for copy in copies:
        copy.wait()
    piece = x_ref[...]
    for side, (wk, wv) in enumerate(((wk_ref, wv_ref), (wkp_ref, wvp_ref))):
        owner = core if side == 0 else 1 - core
        keys = rounded(jnp.dot(piece, wk[...], preferred_element_type=jnp.float32))
        keys = rotated(keys, cos_ref[...], sin_ref[...])
        values = jnp.dot(piece, wv[...], preferred_element_type=jnp.float32)
        for b in range(HALF_BLOCKS):
            rows = slice(b * BLK, (b + 1) * BLK)
            turned = values[rows].T
            for j in range(2):
                cols = slice(j * HEAD_DIM, (j + 1) * HEAD_DIM)
                held[2 * owner + j, b] = jnp.concatenate(
                    [keys[rows, cols], turned[cols]], axis=1
                ).astype(jnp.bfloat16)
    for r in range(CHIPS):
        outs[r][...] = held[lax.rem(chip + r, CHIPS)]


def q_kernel(where_ref, x_hbm, wq_hbm, wqp_ref, cos_ref, sin_ref, picks_ref, *rest):
    outs, (x_ref, wq_ref, held, sems) = rest[:CHIPS], rest[CHIPS:]
    copies = fetch_all([(x_hbm, x_ref), (wq_hbm, wq_ref)], sems)
    core, chip = where_ref[0], where_ref[1]
    rows = x_ref.shape[0]
    for copy in copies:
        copy.wait()
    piece = x_ref[...]
    for side, wq in enumerate((wq_ref, wqp_ref)):
        owner = core if side == 0 else 1 - core
        for j in range(2):
            for t in range(2):
                cols = slice((2 * j + t) * LANES, (2 * j + t + 1) * LANES)
                tile = rounded(jnp.dot(piece, wq[:, cols], preferred_element_type=jnp.float32))
                tile = rotated(tile, cos_ref[...], sin_ref[...]).astype(jnp.bfloat16)
                held[2 * owner + j, :, t * LANES : (t + 1) * LANES] = tile * jnp.bfloat16(
                    HEAD_DIM**-0.5
                )
    mine = jnp.where(core == 0, picks_ref[:HALF_BLOCKS, :], picks_ref[HALF_BLOCKS:, :])
    mine = jnp.concatenate(
        [mine.astype(jnp.float32), jnp.zeros((EXTRA - HALF_BLOCKS, LANES), jnp.float32)], axis=0
    ).astype(jnp.bfloat16)
    for r in range(CHIPS):
        outs[r][:rows, :] = held[lax.rem(chip + r, CHIPS)]
        outs[r][rows:, :LANES] = mine
        outs[r][rows:, LANES:] = jnp.zeros_like(mine)


def assemble_kernel(places, *refs):
    pieces = refs[: len(places)]
    out_ref, sems = refs[-2:]
    copies = fetch_all(
        [
            (piece, out_ref.at[pl.ds(place, piece.shape[0])])
            for piece, place in zip(pieces, places)
        ],
        sems,
    )
    for copy in copies:
        copy.wait()


def attend_kernel(slots_ref, bias_ref, q_ref, held, out_ref, logs_held):
    rows = out_ref.shape[0] - EXTRA
    logs_held[...] = jnp.zeros_like(logs_held)

    left = lax.broadcasted_iota(jnp.int32, (BLK, LANES), 1) < HEAD_DIM
    key_pos = lax.broadcasted_iota(jnp.int32, (BLK, 4 * BLK), 0)
    query_pos = lax.broadcasted_iota(jnp.int32, (BLK, 4 * BLK), 1) % BLK
    causal = key_pos <= query_pos
    left_row = lax.broadcasted_iota(jnp.int32, (1, LANES), 1) < HEAD_DIM

    def one_block(row, start):
        tiles = q_ref[pl.ds(start, BLK), :].astype(jnp.float32)
        heads = []
        for g in range(4):
            tile = tiles[:, (g // 2) * LANES : (g // 2 + 1) * LANES]
            if g % 2 == 1:
                tile = pltpu.roll(tile, HEAD_DIM, 1)
            heads.append(jnp.where(left, tile, 0.0).astype(jnp.bfloat16))
        stacked = jnp.concatenate(heads, axis=0)
        tops, totals, mixes = [], [], []
        for c in range(0, PICK + 1, CHUNK):
            blocks = [held[slots_ref[row, p]] for p in range(c, c + CHUNK)]
            scores = lax.dot_general(
                jnp.concatenate(blocks, axis=0),
                stacked,
                (((1,), (1,)), ((), ())),
                preferred_element_type=jnp.float32,
            )
            parts = [scores[n * BLK : (n + 1) * BLK] for n in range(CHUNK)]
            if c + CHUNK > PICK:
                parts[-1] = jnp.where(causal, parts[-1], NEGATIVE)
            biases = [bias_ref[row, c + n] for n in range(CHUNK)]
            top = None
            for part, extra in zip(parts, biases):
                own_top = jnp.max(part, axis=0, keepdims=True) + extra
                top = own_top if top is None else jnp.maximum(top, own_top)
            parts = [jnp.exp(part - (top - extra)) for part, extra in zip(parts, biases)]
            exponent = jnp.concatenate(parts, axis=0)
            turned = []
            for n in range(0, CHUNK, 2):
                moved = pltpu.roll(blocks[n], HEAD_DIM, 1)
                turned.append(jnp.where(left, moved, blocks[n + 1]))
            tops.append(top)
            totals.append(jnp.sum(exponent, axis=0, keepdims=True))
            mixes.append(
                jnp.dot(
                    jnp.concatenate(turned, axis=1),
                    exponent.astype(jnp.bfloat16),
                    preferred_element_type=jnp.float32,
                )
            )
        top = functools.reduce(jnp.maximum, tops)
        shares = [jnp.exp(one - top) for one in tops]
        total = functools.reduce(jnp.add, [w * one for w, one in zip(shares, totals)])
        inverse = 1.0 / total
        mixed = functools.reduce(
            jnp.add, [(w * inverse) * one for w, one in zip(shares, mixes)]
        )
        flat = []
        for t in range(2):
            tile = mixed[:, t * LANES : (t + 1) * LANES].T
            flat.append(jnp.concatenate([tile[:HEAD_DIM], tile[HEAD_DIM:]], axis=1))
        return jnp.concatenate(flat, axis=1).astype(jnp.bfloat16), top + jnp.log(total)

    def pair(p, carry):
        logs = []
        for u in range(2):
            start = pl.multiple_of((2 * p + u) * BLK, BLK)
            att, log = one_block(2 * p + u, start)
            out_ref[pl.ds(start, BLK), :] = att
            logs.append(log)
        place = pl.ds(pl.multiple_of(p * LANES, LANES), LANES)
        for t in range(2):
            one = logs[0][:, t * LANES : (t + 1) * LANES]
            two = logs[1][:, t * LANES : (t + 1) * LANES]
            pieces_of = (
                jnp.where(left_row, one, pltpu.roll(two, HEAD_DIM, 1)),
                jnp.where(left_row, pltpu.roll(one, HEAD_DIM, 1), two),
            )
            for j, log in enumerate(pieces_of):
                head = 2 * t + j
                high = rounded(log)
                middle = rounded(log - high)
                low = log - high - middle
                for k, part in enumerate((high, middle, low)):
                    logs_held[4 * k + head : 4 * k + head + 1, place] = part
        return carry

    lax.fori_loop(0, HALF_BLOCKS // 2, pair, 0)
    out_ref[rows:, :] = logs_held[...].astype(jnp.bfloat16)


def lse_kernel(where_ref, *rest):
    pieces, keep_ref, give_ref, held = rest[:4], rest[4], rest[5], rest[6]
    core, chip = where_ref[0], where_ref[1]
    for r in range(CHIPS):
        parts = pieces[r][...].astype(jnp.float32)
        held[lax.rem(chip + r, CHIPS)] = parts[0:4] + parts[4:8] + parts[8:12]
    for j in range(2):
        keep_ref[4 * j : 4 * j + 4, :] = held[2 * core + j]
        give_ref[4 * j : 4 * j + 4, :] = held[2 * (1 - core) + j]


def finish_kernel(where_ref, *rest):
    pieces, w_ref, wp_ref, out_ref, held = rest[:4], rest[4], rest[5], rest[6], rest[7]
    core, chip = where_ref[0], where_ref[1]
    rows, width = held.shape[1:]
    for r in range(CHIPS):
        held[lax.rem(chip + r, CHIPS)] = pieces[r][:rows, :]
    projected = None
    for side, w in enumerate((w_ref, wp_ref)):
        owner = core if side == 0 else 1 - core
        for j in range(2):
            term = jnp.dot(
                held[2 * owner + j],
                w[j * width : (j + 1) * width, :],
                preferred_element_type=jnp.float32,
            )
            projected = term if projected is None else projected + term
    scale = lax.rsqrt(jnp.mean(projected * projected, axis=1, keepdims=True) + EPSILON)
    out_ref[...] = (projected * scale).astype(jnp.bfloat16)


SMEM = pl.BlockSpec(memory_space=pltpu.SMEM)
VMEM = pl.BlockSpec(memory_space=pltpu.VMEM)
ANY = pl.BlockSpec(memory_space=pl.ANY)
HBM = pl.BlockSpec(memory_space=pltpu.HBM)


def grant(mib):
    return pltpu.CompilerParams(vmem_limit_bytes=mib * 2**20)


def assemble(pieces, places, total, before=None):
    moved = sum(p.size * 2 for p in pieces)
    resumed = before is not None
    return pl.pallas_call(
        functools.partial(assemble_kernel, places),
        in_specs=[ANY] * (len(pieces) + resumed),
        out_specs=ANY,
        out_shape=pltpu.VMEM((total, BLK, LANES), jnp.bfloat16),
        scratch_shapes=[pltpu.SemaphoreType.DMA((len(pieces),))],
        input_output_aliases={len(pieces): 0} if resumed else {},
        cost_estimate=pl.CostEstimate(
            flops=moved * 100, bytes_accessed=2 * moved, transcendentals=0
        ),
        compiler_params=grant(8),
        name="assemble",
    )(*pieces, *([before] if resumed else []))


def attend(slots, bias, queries, held):
    rows, width = queries.shape[0] - EXTRA, queries.shape[1]
    return pl.pallas_call(
        attend_kernel,
        in_specs=[SMEM, SMEM, VMEM, VMEM],
        out_specs=VMEM,
        out_shape=pltpu.VMEM((rows + EXTRA, width), jnp.bfloat16),
        scratch_shapes=[pltpu.VMEM((EXTRA, rows), jnp.float32)],
        cost_estimate=pl.CostEstimate(
            flops=32 * rows * width * (PICK + 1) * BLK,
            bytes_accessed=rows * (PICK + 1) * LANES * 2,
            transcendentals=0,
        ),
        compiler_params=grant(16),
        name="attend",
    )(slots, bias, queries, held)


def tied(value, *others):
    return lax.optimization_barrier((value,) + others)[0]


def shards(tokens, w_query, w_key, w_value, w_out, chosen):
    core = lax.axis_index("tp")
    index = lax.axis_index("kv")
    planes = lax.axis_size("kv") // CHIPS
    plane, chip = index // CHIPS, index % CHIPS
    here = jnp.stack([core, chip]).astype(jnp.int32)

    def partner(x):
        return lax.ppermute(x, "tp", [(0, 1), (1, 0)])

    def along_y(x, r):
        return lax.ppermute(
            x,
            "kv",
            [
                (z * CHIPS + y, z * CHIPS + (y + r) % CHIPS)
                for z in range(planes)
                for y in range(CHIPS)
            ],
        )

    def hop(x):
        pairs = []
        for z in range(planes):
            for y in range(CHIPS):
                for c, step in enumerate((1, -1)):
                    to = (z + step) % planes
                    pairs.append(((z * CHIPS + y) * 2 + c, (to * CHIPS + y) * 2 + c))
        return lax.ppermute(x, ("kv", "tp"), pairs)

    own = tokens[0]
    rows = own.shape[0]
    wk_peer, wv_peer = partner(w_key), partner(w_value)
    wq_peer = partner(tied(w_query, wk_peer, wv_peer))
    wo_peer = partner(tied(w_out, wk_peer, wv_peer))

    own_v, wk_v, wv_v = pl.pallas_call(
        preload_kernel,
        in_specs=[HBM] * 3,
        out_specs=[ANY] * 3,
        out_shape=[pltpu.VMEM(x.shape, jnp.bfloat16) for x in (own, w_key, w_value)],
        scratch_shapes=[pltpu.SemaphoreType.DMA((3,))],
        compiler_params=grant(60),
        name="preload",
    )(own, w_key, w_value)
    base = index * 2 * rows + core * rows
    cosine, sine = rotary_tables(base + jnp.arange(rows, dtype=jnp.int32))

    width = own.shape[1]
    piece_shape = (HALF_BLOCKS, BLK, LANES)
    kv_out = pl.pallas_call(
        kv_kernel,
        in_specs=[SMEM] + [ANY] * 3 + [VMEM] * 4,
        out_specs=[VMEM] * CHIPS,
        out_shape=[pltpu.VMEM(piece_shape, jnp.bfloat16)] * CHIPS,
        scratch_shapes=[
            pltpu.VMEM((rows, width), jnp.bfloat16),
            pltpu.VMEM(w_key.shape, jnp.bfloat16),
            pltpu.VMEM(w_value.shape, jnp.bfloat16),
            pltpu.VMEM((CHIPS,) + piece_shape, jnp.bfloat16),
            pltpu.SemaphoreType.DMA((3,)),
        ],
        compiler_params=grant(8),
        name="project_kv",
    )(here, own_v, wk_v, wv_v, wk_peer, wv_peer, cosine, sine)
    kv_in = [kv_out[0]] + [along_y(kv_out[r], r) for r in range(1, CHIPS)]

    q_shape = (rows + EXTRA, 4 * HEAD_DIM)
    q_out = pl.pallas_call(
        q_kernel,
        in_specs=[SMEM] + [HBM] * 2 + [VMEM] * 4,
        out_specs=[VMEM] * CHIPS,
        out_shape=[pltpu.VMEM(q_shape, jnp.bfloat16)] * CHIPS,
        scratch_shapes=[
            pltpu.VMEM((rows, width), jnp.bfloat16),
            pltpu.VMEM(w_query.shape, jnp.bfloat16),
            pltpu.VMEM((CHIPS, rows, 4 * HEAD_DIM), jnp.bfloat16),
            pltpu.SemaphoreType.DMA((2,)),
        ],
        compiler_params=grant(10),
        name="project_q",
    )(
        here,
        own,
        w_query,
        wq_peer,
        tied(cosine, kv_out[0]),
        sine,
        jnp.pad(chosen[0], ((0, 0), (0, LANES - PICK))),
    )
    chunk = CHIPS * HALF_BLOCKS
    mine = jnp.concatenate(kv_in, axis=0)
    both = jnp.concatenate([mine, partner(mine)], axis=0)

    last = planes // 2
    ring, swapped = {0: both}, {}
    q_in = [q_out[0]]
    for n in range(1, last + 1):
        moving = ring[n - 1]
        if n == 2:
            moving, *q_ready = lax.optimization_barrier((moving,) + tuple(q_out))
            q_in = [q_ready[0]] + [along_y(q_ready[r], r) for r in range(1, CHIPS)]
            swapped[1] = partner(moving)
        if n == 3:
            swapped[2] = partner(moving)
            moving, swapped[1], *q_in = lax.optimization_barrier(
                (moving, swapped[1]) + tuple(q_in)
            )
        ring[n] = hop(moving if n < last else moving[:chunk])
    if last < 2:
        q_in = [q_out[0]] + [along_y(q_out[r], r) for r in range(1, CHIPS)]
    for n in range(1, last):
        if n not in swapped:
            swapped[n] = partner(ring[n])

    total = 2 * planes * chunk
    early = [(ring[n], 2 * n * chunk) for n in range(last)]
    early += [(swapped[n], 2 * (planes - n) * chunk) for n in range(1, last)]
    held = assemble([p for p, _ in early], [at for _, at in early], total)
    late = [ring[last], partner(ring[last])]
    held = assemble(late, [2 * last * chunk, (2 * last + 1) * chunk], total, held)

    picks = jnp.stack([q[rows : rows + HALF_BLOCKS, :PICK] for q in q_in]).astype(jnp.int32)
    shift = jnp.arange(CHIPS, dtype=jnp.int32)
    source = (chip - shift) % CHIPS
    own_block = (
        plane * (8 * CHIPS)
        + source[:, None] * 8
        + core * HALF_BLOCKS
        + jnp.arange(HALF_BLOCKS, dtype=jnp.int32)[None, :]
    )
    blocks = jnp.concatenate([picks, own_block[:, :, None]], axis=2)
    bias = jnp.where(blocks >= 0, 0.0, NEGATIVE).astype(jnp.float32)
    blocks = jnp.maximum(blocks, 0)
    half = blocks // HALF_BLOCKS % 2
    distance = (plane - blocks // (8 * CHIPS)) % planes
    turn = (chip - blocks // 8 % CHIPS) % CHIPS
    place = jnp.where(core == 0, distance, (planes - distance) % planes)
    half = jnp.where(
        distance % last == 0, half ^ core, jnp.where(distance < last, half, 1 - half)
    )
    slots = ((place * 2 + half) * CHIPS + turn) * HALF_BLOCKS + blocks % HALF_BLOCKS

    att = {}
    for r in (2, 1, 3, 0):
        done = attend(slots[r], bias[r], q_in[r], held)
        att[r] = along_y(done, -r) if r else done

    tail = rows // EXTRA
    keep, give = pl.pallas_call(
        lse_kernel,
        grid=(1,),
        in_specs=[SMEM] + [pl.BlockSpec((EXTRA, rows), lambda i: (tail, 0))] * CHIPS,
        out_specs=[pl.BlockSpec((8, rows), lambda i: (0, 0))] * 2,
        out_shape=[jax.ShapeDtypeStruct((8, rows), jnp.float32)] * 2,
        scratch_shapes=[pltpu.VMEM((CHIPS, 4, rows), jnp.float32)],
        compiler_params=grant(4),
        name="sort_logsums",
    )(here, *[att[r] for r in range(CHIPS)])
    got = partner(give)
    normed = pl.pallas_call(
        finish_kernel,
        in_specs=[SMEM] + [VMEM] * (CHIPS + 2),
        out_specs=VMEM,
        out_shape=jax.ShapeDtypeStruct((rows, w_out.shape[1]), jnp.bfloat16),
        scratch_shapes=[pltpu.VMEM((CHIPS, rows, 4 * HEAD_DIM), jnp.bfloat16)],
        compiler_params=grant(10),
        name="finish",
    )(here, *[att[r] for r in range(CHIPS)], w_out, wo_peer)
    first = jnp.where(core == 0, keep, got)
    second = jnp.where(core == 0, got, keep)
    logsums = jnp.concatenate([first, second], axis=1).T
    return (normed[None], logsums[None])


def solution(mesh):
    placed = (
        P("dp", ("kv", "tp"), None),
        P(None, "tp"),
        P(None, "tp"),
        P(None, "tp"),
        P("tp", None),
        P("dp", "kv", None),
    )
    return jax.shard_map(
        shards,
        mesh=mesh,
        in_specs=placed,
        out_specs=(P("dp", ("kv", "tp"), None), P("dp", "kv", "tp")),
        check_vma=False,
    )
```

```python
import functools

import jax
import jax.numpy as jnp
from jax import lax
from jax.experimental import pallas as pl
from jax.experimental.pallas import tpu as pltpu
from jax.sharding import PartitionSpec as P

HEAD_DIM = 64
BLK = 64
PICK = 15
THETA_BASE = 10000.0
NEGATIVE = -1e30
EPSILON = 1e-06
LANES = 128
CHIPS = 4
HALF_BLOCKS = 4
EXTRA = 16


def rotary_tables(positions):
    half = HEAD_DIM // 2
    inverse = THETA_BASE ** (-jnp.arange(half, dtype=jnp.float32) / half)
    angles = positions.astype(jnp.float32)[:, None] * inverse[None, :]
    cosine = jnp.cos(angles)
    sine = jnp.sin(angles)
    return (
        jnp.concatenate([cosine] * 4, axis=1),
        jnp.concatenate([-sine, sine, -sine, sine], axis=1),
    )


def rotated(values, cosine, sine):
    lane = lax.broadcasted_iota(jnp.int32, values.shape, 1)
    ahead = pltpu.roll(values, LANES - HEAD_DIM // 2, 1)
    behind = pltpu.roll(values, HEAD_DIM // 2, 1)
    swapped = jnp.where(lane % HEAD_DIM < HEAD_DIM // 2, ahead, behind)
    return values * cosine + swapped * sine


def rounded(x):
    return x.astype(jnp.bfloat16).astype(jnp.float32)


def kv_kernel(where_ref, x_ref, wk_ref, wkp_ref, wv_ref, wvp_ref, cos_ref, sin_ref, *rest):
    outs, held = rest[:-1], rest[-1]
    core, chip = where_ref[0], where_ref[1]
    piece = x_ref[...]
    for side, (wk, wv) in enumerate(((wk_ref, wv_ref), (wkp_ref, wvp_ref))):
        owner = core if side == 0 else 1 - core
        keys = rounded(jnp.dot(piece, wk[...], preferred_element_type=jnp.float32))
        keys = rotated(keys, cos_ref[...], sin_ref[...])
        values = jnp.dot(piece, wv[...], preferred_element_type=jnp.float32)
        for b in range(HALF_BLOCKS):
            rows = slice(b * BLK, (b + 1) * BLK)
            turned = values[rows].T
            for j in range(2):
                cols = slice(j * HEAD_DIM, (j + 1) * HEAD_DIM)
                held[2 * owner + j, b] = jnp.concatenate(
                    [keys[rows, cols], turned[cols]], axis=1
                ).astype(jnp.bfloat16)
    for r in range(CHIPS):
        outs[r][...] = held[lax.rem(chip + r, CHIPS)]


def q_kernel(where_ref, x_ref, wq_ref, wqp_ref, cos_ref, sin_ref, picks_ref, *rest):
    outs, held = rest[:-1], rest[-1]
    core, chip = where_ref[0], where_ref[1]
    piece = x_ref[...]
    rows = piece.shape[0]
    for side, wq in enumerate((wq_ref, wqp_ref)):
        owner = core if side == 0 else 1 - core
        for j in range(2):
            for t in range(2):
                cols = slice((2 * j + t) * LANES, (2 * j + t + 1) * LANES)
                tile = rounded(jnp.dot(piece, wq[:, cols], preferred_element_type=jnp.float32))
                tile = rotated(tile, cos_ref[...], sin_ref[...]).astype(jnp.bfloat16)
                held[2 * owner + j, :, t * LANES : (t + 1) * LANES] = tile * jnp.bfloat16(
                    HEAD_DIM**-0.5
                )
    mine = jnp.where(core == 0, picks_ref[:HALF_BLOCKS, :], picks_ref[HALF_BLOCKS:, :])
    mine = jnp.concatenate(
        [mine.astype(jnp.float32), jnp.zeros((EXTRA - HALF_BLOCKS, LANES), jnp.float32)], axis=0
    ).astype(jnp.bfloat16)
    for r in range(CHIPS):
        outs[r][:rows, :] = held[lax.rem(chip + r, CHIPS)]
        outs[r][rows:, :LANES] = mine
        outs[r][rows:, LANES:] = jnp.zeros_like(mine)


def attend_kernel(count, planes, slots_ref, bias_ref, *rest):
    queries = rest[:count]
    pieces = rest[count : count + 2 * planes]
    outs = rest[count + 2 * planes : 2 * count + 2 * planes]
    held, asked, told, logs_held, sem = rest[2 * count + 2 * planes :]
    rows = outs[0].shape[0] - EXTRA
    chunk = CHIPS * HALF_BLOCKS

    copies = [
        pltpu.make_async_copy(piece, held.at[pl.ds(n * chunk, chunk)], sem.at[n])
        for n, piece in enumerate(pieces)
    ]
    for copy in copies:
        copy.start()
    for n in range(count):
        asked[n] = queries[n][:rows, :]
    logs_held[...] = jnp.zeros_like(logs_held)
    for copy in copies:
        copy.wait()

    left = lax.broadcasted_iota(jnp.int32, (BLK, LANES), 1) < HEAD_DIM
    key_pos = lax.broadcasted_iota(jnp.int32, (BLK, 4 * BLK), 0)
    query_pos = lax.broadcasted_iota(jnp.int32, (BLK, 4 * BLK), 1) % BLK
    causal = key_pos <= query_pos
    left_row = lax.broadcasted_iota(jnp.int32, (1, LANES), 1) < HEAD_DIM

    def one_block(n, row, start):
        tiles = asked[n, pl.ds(start, BLK), :].astype(jnp.float32)
        heads = []
        for g in range(4):
            tile = tiles[:, (g // 2) * LANES : (g // 2 + 1) * LANES]
            if g % 2 == 1:
                tile = pltpu.roll(tile, HEAD_DIM, 1)
            heads.append(jnp.where(left, tile, 0.0).astype(jnp.bfloat16))
        stacked = jnp.concatenate(heads, axis=0)
        blocks = [held[slots_ref[row, p]] for p in range(PICK + 1)]
        scores = lax.dot_general(
            jnp.concatenate(blocks, axis=0),
            stacked,
            (((1,), (1,)), ((), ())),
            preferred_element_type=jnp.float32,
        )
        parts = [scores[p * BLK : (p + 1) * BLK] for p in range(PICK + 1)]
        parts[PICK] = jnp.where(causal, parts[PICK], NEGATIVE)
        biases = [bias_ref[row, p] for p in range(PICK + 1)]
        top = functools.reduce(
            jnp.maximum,
            [jnp.max(x, axis=0, keepdims=True) + extra for x, extra in zip(parts, biases)],
        )
        exponent = jnp.concatenate(
            [jnp.exp(x - (top - extra)) for x, extra in zip(parts, biases)], axis=0
        )
        total = jnp.sum(exponent, axis=0, keepdims=True)
        turned = [
            jnp.where(left, pltpu.roll(blocks[p], HEAD_DIM, 1), blocks[p + 1])
            for p in range(0, PICK + 1, 2)
        ]
        mixed = jnp.dot(
            jnp.concatenate(turned, axis=1),
            exponent.astype(jnp.bfloat16),
            preferred_element_type=jnp.float32,
        )
        mixed = mixed * (1.0 / total)
        flat = []
        for t in range(2):
            tile = mixed[:, t * LANES : (t + 1) * LANES].T
            flat.append(jnp.concatenate([tile[:HEAD_DIM], tile[HEAD_DIM:]], axis=1))
        return jnp.concatenate(flat, axis=1).astype(jnp.bfloat16), top + jnp.log(total)

    def pair(step, carry):
        n, p = lax.div(step, HALF_BLOCKS // 2), lax.rem(step, HALF_BLOCKS // 2)
        logs = []
        for u in range(2):
            start = pl.multiple_of((2 * p + u) * BLK, BLK)
            att, log = one_block(n, 2 * step + u, start)
            told[n, pl.ds(start, BLK), :] = att
            logs.append(log)
        place = pl.ds(pl.multiple_of(p * LANES, LANES), LANES)
        for t in range(2):
            one = logs[0][:, t * LANES : (t + 1) * LANES]
            two = logs[1][:, t * LANES : (t + 1) * LANES]
            pieces_of = (
                jnp.where(left_row, one, pltpu.roll(two, HEAD_DIM, 1)),
                jnp.where(left_row, pltpu.roll(one, HEAD_DIM, 1), two),
            )
            for j, log in enumerate(pieces_of):
                head = 2 * t + j
                high = rounded(log)
                middle = rounded(log - high)
                low = log - high - middle
                for k, part in enumerate((high, middle, low)):
                    logs_held[n, 4 * k + head : 4 * k + head + 1, place] = part
        return carry

    lax.fori_loop(0, count * HALF_BLOCKS // 2, pair, 0)
    for n in range(count):
        outs[n][:rows, :] = told[n]
        outs[n][rows:, :] = logs_held[n].astype(jnp.bfloat16)


def lse_kernel(where_ref, *rest):
    pieces, keep_ref, give_ref, held = rest[:4], rest[4], rest[5], rest[6]
    core, chip = where_ref[0], where_ref[1]
    for r in range(CHIPS):
        parts = pieces[r][...].astype(jnp.float32)
        held[lax.rem(chip + r, CHIPS)] = parts[0:4] + parts[4:8] + parts[8:12]
    for j in range(2):
        keep_ref[4 * j : 4 * j + 4, :] = held[2 * core + j]
        give_ref[4 * j : 4 * j + 4, :] = held[2 * (1 - core) + j]


def finish_kernel(where_ref, *rest):
    pieces, w_ref, wp_ref, out_ref, held = rest[:4], rest[4], rest[5], rest[6], rest[7]
    core, chip = where_ref[0], where_ref[1]
    rows, width = held.shape[1:]
    for r in range(CHIPS):
        held[lax.rem(chip + r, CHIPS)] = pieces[r][:rows, :]
    projected = None
    for side, w in enumerate((w_ref, wp_ref)):
        owner = core if side == 0 else 1 - core
        for j in range(2):
            term = jnp.dot(
                held[2 * owner + j],
                w[j * width : (j + 1) * width, :],
                preferred_element_type=jnp.float32,
            )
            projected = term if projected is None else projected + term
    scale = lax.rsqrt(jnp.mean(projected * projected, axis=1, keepdims=True) + EPSILON)
    out_ref[...] = (projected * scale).astype(jnp.bfloat16)


SMEM = pl.BlockSpec(memory_space=pltpu.SMEM)
VMEM = pl.BlockSpec(memory_space=pltpu.VMEM)
ANY = pl.BlockSpec(memory_space=pl.ANY)


def grant(mib):
    return pltpu.CompilerParams(vmem_limit_bytes=mib * 2**20)


def attend(planes, slots, bias, queries, pieces):
    count = len(queries)
    rows, width = queries[0].shape[0] - EXTRA, queries[0].shape[1]
    total = 2 * planes * CHIPS * HALF_BLOCKS
    return pl.pallas_call(
        functools.partial(attend_kernel, count, planes),
        in_specs=[SMEM, SMEM] + [VMEM] * count + [ANY] * len(pieces),
        out_specs=[VMEM] * count,
        out_shape=[jax.ShapeDtypeStruct((rows + EXTRA, width), jnp.bfloat16)] * count,
        scratch_shapes=[
            pltpu.VMEM((total, BLK, LANES), jnp.bfloat16),
            pltpu.VMEM((count, rows, width), jnp.bfloat16),
            pltpu.VMEM((count, rows, width), jnp.bfloat16),
            pltpu.VMEM((count, EXTRA, rows), jnp.float32),
            pltpu.SemaphoreType.DMA((len(pieces),)),
        ],
        cost_estimate=pl.CostEstimate(
            flops=count * 32 * rows * width * (PICK + 1) * BLK,
            bytes_accessed=total * BLK * LANES * 2,
            transcendentals=0,
        ),
        compiler_params=grant(16),
        name="attend",
    )(slots, bias, *queries, *pieces)


def tied(value, *others):
    return lax.optimization_barrier((value,) + others)[0]


def shards(tokens, w_query, w_key, w_value, w_out, chosen):
    core = lax.axis_index("tp")
    index = lax.axis_index("kv")
    planes = lax.axis_size("kv") // CHIPS
    plane, chip = index // CHIPS, index % CHIPS
    here = jnp.stack([core, chip]).astype(jnp.int32)

    def partner(x):
        return lax.ppermute(x, "tp", [(0, 1), (1, 0)])

    def along_y(x, r):
        return lax.ppermute(
            x,
            "kv",
            [
                (z * CHIPS + y, z * CHIPS + (y + r) % CHIPS)
                for z in range(planes)
                for y in range(CHIPS)
            ],
        )

    def along_z(x, step):
        return lax.ppermute(
            x,
            "kv",
            [
                (z * CHIPS + y, (z + step) % planes * CHIPS + y)
                for z in range(planes)
                for y in range(CHIPS)
            ],
        )

    own = tokens[0]
    rows = own.shape[0]
    wk_peer, wv_peer = partner(w_key), partner(w_value)
    wq_peer = partner(tied(w_query, wk_peer, wv_peer))

    base = index * 2 * rows + core * rows
    cosine, sine = rotary_tables(base + jnp.arange(rows, dtype=jnp.int32))

    piece_shape = (HALF_BLOCKS, BLK, LANES)
    kv_out = pl.pallas_call(
        kv_kernel,
        in_specs=[SMEM] + [VMEM] * 7,
        out_specs=[VMEM] * CHIPS,
        out_shape=[jax.ShapeDtypeStruct(piece_shape, jnp.bfloat16)] * CHIPS,
        scratch_shapes=[pltpu.VMEM((CHIPS,) + piece_shape, jnp.bfloat16)],
        compiler_params=grant(8),
        name="project_kv",
    )(here, own, w_key, wk_peer, w_value, wv_peer, cosine, sine)
    kv_in = [kv_out[0]] + [along_y(kv_out[r], r) for r in range(1, CHIPS)]

    q_shape = (rows + EXTRA, 4 * HEAD_DIM)
    q_out = pl.pallas_call(
        q_kernel,
        in_specs=[SMEM] + [VMEM] * 6,
        out_specs=[VMEM] * CHIPS,
        out_shape=[jax.ShapeDtypeStruct(q_shape, jnp.bfloat16)] * CHIPS,
        scratch_shapes=[pltpu.VMEM((CHIPS, rows, 4 * HEAD_DIM), jnp.bfloat16)],
        compiler_params=grant(10),
        name="project_q",
    )(
        here,
        own,
        w_query,
        wq_peer,
        tied(cosine, kv_out[0]),
        sine,
        jnp.pad(chosen[0], ((0, 0), (0, LANES - PICK))),
    )
    start = jnp.stack(kv_in)

    chunks = {0: start}
    order = [0]
    up = down = start
    for n in range(1, planes // 2 + 1):
        if n == 2:
            up, down, *q_out = lax.optimization_barrier((up, down) + tuple(q_out))
        up = along_z(up, 1)
        chunks[n] = up
        order.append(n)
        if n <= planes - 1 - planes // 2:
            down = along_z(down, -1)
            chunks[planes - n] = down
            order.append(planes - n)
    q_ready = [tied(q_out[r], chunks[planes // 2]) for r in range(CHIPS)]
    q_in = [q_ready[0]] + [along_y(q_ready[r], r) for r in range(1, CHIPS)]
    wo_peer = partner(tied(w_out, chunks[1]))

    flat = (CHIPS * HALF_BLOCKS, BLK, LANES)
    swapped = {}
    for at, d in enumerate(order):
        later = order[min(at + 2, len(order) - 1)]
        value = chunks[d] if later == d else tied(chunks[d], chunks[later])
        swapped[d] = partner(value)
    pieces = [chunks[d].reshape(flat) for d in range(planes)]
    pieces += [swapped[d].reshape(flat) for d in range(planes)]

    picks = jnp.stack([q[rows : rows + HALF_BLOCKS, :PICK] for q in q_in]).astype(jnp.int32)
    shift = jnp.arange(CHIPS, dtype=jnp.int32)
    source = (chip - shift) % CHIPS
    own_block = (
        plane * (8 * CHIPS)
        + source[:, None] * 8
        + core * HALF_BLOCKS
        + jnp.arange(HALF_BLOCKS, dtype=jnp.int32)[None, :]
    )
    blocks = jnp.concatenate([picks, own_block[:, :, None]], axis=2)
    bias = jnp.where(blocks >= 0, 0.0, NEGATIVE).astype(jnp.float32)
    blocks = jnp.maximum(blocks, 0)
    flag = (blocks // HALF_BLOCKS % 2) ^ core
    distance = (plane - blocks // (8 * CHIPS)) % planes
    turn = (chip - blocks // 8 % CHIPS) % CHIPS
    slots = ((flag * planes + distance) * CHIPS + turn) * HALF_BLOCKS + blocks % HALF_BLOCKS

    att = {}
    for shifts in ((2, 1, 3), (0,)):
        span = slice(1, None) if len(shifts) > 1 else slice(0, 1)
        names = sorted(shifts)
        done = attend(
            planes,
            slots[span].reshape(-1, PICK + 1),
            bias[span].reshape(-1, PICK + 1),
            [q_in[r] for r in names],
            pieces,
        )
        for n, r in enumerate(names):
            att[r] = along_y(done[n], -r) if r else done[n]

    tail = rows // EXTRA
    keep, give = pl.pallas_call(
        lse_kernel,
        grid=(1,),
        in_specs=[SMEM] + [pl.BlockSpec((EXTRA, rows), lambda i: (tail, 0))] * CHIPS,
        out_specs=[pl.BlockSpec((8, rows), lambda i: (0, 0))] * 2,
        out_shape=[jax.ShapeDtypeStruct((8, rows), jnp.float32)] * 2,
        scratch_shapes=[pltpu.VMEM((CHIPS, 4, rows), jnp.float32)],
        compiler_params=grant(4),
        name="sort_logsums",
    )(here, *[att[r] for r in range(CHIPS)])
    got = partner(give)
    normed = pl.pallas_call(
        finish_kernel,
        in_specs=[SMEM] + [VMEM] * (CHIPS + 2),
        out_specs=VMEM,
        out_shape=jax.ShapeDtypeStruct((rows, w_out.shape[1]), jnp.bfloat16),
        scratch_shapes=[pltpu.VMEM((CHIPS, rows, 4 * HEAD_DIM), jnp.bfloat16)],
        compiler_params=grant(10),
        name="finish",
    )(here, *[att[r] for r in range(CHIPS)], w_out, wo_peer)
    first = jnp.where(core == 0, keep, got)
    second = jnp.where(core == 0, got, keep)
    logsums = jnp.concatenate([first, second], axis=1).T
    return (normed[None], logsums[None])


def solution(mesh):
    placed = (
        P("dp", ("kv", "tp"), None),
        P(None, "tp"),
        P(None, "tp"),
        P(None, "tp"),
        P("tp", None),
        P("dp", "kv", None),
    )
    return jax.shard_map(
        shards,
        mesh=mesh,
        in_specs=placed,
        out_specs=(P("dp", ("kv", "tp"), None), P("dp", "kv", "tp")),
        check_vma=False,
    )
```

```python
import functools

import jax
import jax.numpy as jnp
from jax import lax
from jax.experimental import pallas as pl
from jax.experimental.pallas import tpu as pltpu
from jax.sharding import PartitionSpec as P

HEAD_DIM = 64
BLK = 64
PICK = 15
THETA_BASE = 10000.0
NEGATIVE = -1e30
EPSILON = 1e-06
LANES = 128
CHIPS = 4
HALF_BLOCKS = 4
EXTRA = 16


def rotary_tables(positions):
    half = HEAD_DIM // 2
    inverse = THETA_BASE ** (-jnp.arange(half, dtype=jnp.float32) / half)
    angles = positions.astype(jnp.float32)[:, None] * inverse[None, :]
    cosine = jnp.cos(angles)
    sine = jnp.sin(angles)
    return (
        jnp.concatenate([cosine] * 4, axis=1),
        jnp.concatenate([-sine, sine, -sine, sine], axis=1),
    )


def rotated(values, cosine, sine):
    lane = lax.broadcasted_iota(jnp.int32, values.shape, 1)
    ahead = pltpu.roll(values, LANES - HEAD_DIM // 2, 1)
    behind = pltpu.roll(values, HEAD_DIM // 2, 1)
    swapped = jnp.where(lane % HEAD_DIM < HEAD_DIM // 2, ahead, behind)
    return values * cosine + swapped * sine


def rounded(x):
    return x.astype(jnp.bfloat16).astype(jnp.float32)


def kv_kernel(where_ref, x_ref, wk_ref, wkp_ref, wv_ref, wvp_ref, cos_ref, sin_ref, *rest):
    outs, held = rest[:-1], rest[-1]
    core, chip = where_ref[0], where_ref[1]
    piece = x_ref[...]
    for side, (wk, wv) in enumerate(((wk_ref, wv_ref), (wkp_ref, wvp_ref))):
        owner = core if side == 0 else 1 - core
        keys = rounded(jnp.dot(piece, wk[...], preferred_element_type=jnp.float32))
        keys = rotated(keys, cos_ref[...], sin_ref[...])
        values = jnp.dot(piece, wv[...], preferred_element_type=jnp.float32)
        for b in range(HALF_BLOCKS):
            rows = slice(b * BLK, (b + 1) * BLK)
            turned = values[rows].T
            for j in range(2):
                cols = slice(j * HEAD_DIM, (j + 1) * HEAD_DIM)
                held[2 * owner + j, b] = jnp.concatenate(
                    [keys[rows, cols], turned[cols]], axis=1
                ).astype(jnp.bfloat16)
    for r in range(CHIPS):
        outs[r][...] = held[lax.rem(chip + r, CHIPS)]


def q_kernel(where_ref, x_ref, wq_ref, wqp_ref, cos_ref, sin_ref, picks_ref, *rest):
    outs, held = rest[:-1], rest[-1]
    core, chip = where_ref[0], where_ref[1]
    piece = x_ref[...]
    rows = piece.shape[0]
    for side, wq in enumerate((wq_ref, wqp_ref)):
        owner = core if side == 0 else 1 - core
        for j in range(2):
            for t in range(2):
                cols = slice((2 * j + t) * LANES, (2 * j + t + 1) * LANES)
                tile = rounded(jnp.dot(piece, wq[:, cols], preferred_element_type=jnp.float32))
                tile = rotated(tile, cos_ref[...], sin_ref[...]).astype(jnp.bfloat16)
                held[2 * owner + j, :, t * LANES : (t + 1) * LANES] = tile * jnp.bfloat16(
                    HEAD_DIM**-0.5
                )
    mine = jnp.where(core == 0, picks_ref[:HALF_BLOCKS, :], picks_ref[HALF_BLOCKS:, :])
    mine = jnp.concatenate(
        [mine.astype(jnp.float32), jnp.zeros((EXTRA - HALF_BLOCKS, LANES), jnp.float32)], axis=0
    ).astype(jnp.bfloat16)
    for r in range(CHIPS):
        outs[r][:rows, :] = held[lax.rem(chip + r, CHIPS)]
        outs[r][rows:, :LANES] = mine
        outs[r][rows:, LANES:] = jnp.zeros_like(mine)


def attend_kernel(count, planes, slots_ref, bias_ref, *rest):
    queries = rest[:count]
    pieces = rest[count : count + 2 * planes]
    outs = rest[count + 2 * planes : 2 * count + 2 * planes]
    held, asked, told, logs_held, sem = rest[2 * count + 2 * planes :]
    rows = outs[0].shape[0] - EXTRA
    chunk = CHIPS * HALF_BLOCKS

    copies = [
        pltpu.make_async_copy(piece, held.at[pl.ds(n * chunk, chunk)], sem.at[n])
        for n, piece in enumerate(pieces)
    ]
    for copy in copies:
        copy.start()
    for n in range(count):
        asked[n] = queries[n][:rows, :]
    logs_held[...] = jnp.zeros_like(logs_held)
    for copy in copies:
        copy.wait()

    left = lax.broadcasted_iota(jnp.int32, (BLK, LANES), 1) < HEAD_DIM
    key_pos = lax.broadcasted_iota(jnp.int32, (BLK, 4 * BLK), 0)
    query_pos = lax.broadcasted_iota(jnp.int32, (BLK, 4 * BLK), 1) % BLK
    causal = key_pos <= query_pos
    left_row = lax.broadcasted_iota(jnp.int32, (1, LANES), 1) < HEAD_DIM

    def one_block(n, row, start):
        tiles = asked[n, pl.ds(start, BLK), :].astype(jnp.float32)
        heads = []
        for g in range(4):
            tile = tiles[:, (g // 2) * LANES : (g // 2 + 1) * LANES]
            if g % 2 == 1:
                tile = pltpu.roll(tile, HEAD_DIM, 1)
            heads.append(jnp.where(left, tile, 0.0).astype(jnp.bfloat16))
        stacked = jnp.concatenate(heads, axis=0)
        blocks = [held[slots_ref[row, p]] for p in range(PICK + 1)]
        scores = lax.dot_general(
            jnp.concatenate(blocks, axis=0),
            stacked,
            (((1,), (1,)), ((), ())),
            preferred_element_type=jnp.float32,
        )
        parts = [scores[p * BLK : (p + 1) * BLK] for p in range(PICK + 1)]
        parts[PICK] = jnp.where(causal, parts[PICK], NEGATIVE)
        biases = [bias_ref[row, p] for p in range(PICK + 1)]
        top = functools.reduce(
            jnp.maximum,
            [jnp.max(x, axis=0, keepdims=True) + extra for x, extra in zip(parts, biases)],
        )
        exponent = jnp.concatenate(
            [jnp.exp(x - (top - extra)) for x, extra in zip(parts, biases)], axis=0
        )
        total = jnp.sum(exponent, axis=0, keepdims=True)
        turned = [
            jnp.where(left, pltpu.roll(blocks[p], HEAD_DIM, 1), blocks[p + 1])
            for p in range(0, PICK + 1, 2)
        ]
        mixed = jnp.dot(
            jnp.concatenate(turned, axis=1),
            exponent.astype(jnp.bfloat16),
            preferred_element_type=jnp.float32,
        )
        mixed = mixed * (1.0 / total)
        flat = []
        for t in range(2):
            tile = mixed[:, t * LANES : (t + 1) * LANES].T
            flat.append(jnp.concatenate([tile[:HEAD_DIM], tile[HEAD_DIM:]], axis=1))
        return jnp.concatenate(flat, axis=1).astype(jnp.bfloat16), top + jnp.log(total)

    def pair(step, carry):
        n, p = lax.div(step, HALF_BLOCKS // 2), lax.rem(step, HALF_BLOCKS // 2)
        logs = []
        for u in range(2):
            start = pl.multiple_of((2 * p + u) * BLK, BLK)
            att, log = one_block(n, 2 * step + u, start)
            told[n, pl.ds(start, BLK), :] = att
            logs.append(log)
        place = pl.ds(pl.multiple_of(p * LANES, LANES), LANES)
        for t in range(2):
            one = logs[0][:, t * LANES : (t + 1) * LANES]
            two = logs[1][:, t * LANES : (t + 1) * LANES]
            pieces_of = (
                jnp.where(left_row, one, pltpu.roll(two, HEAD_DIM, 1)),
                jnp.where(left_row, pltpu.roll(one, HEAD_DIM, 1), two),
            )
            for j, log in enumerate(pieces_of):
                head = 2 * t + j
                high = rounded(log)
                middle = rounded(log - high)
                low = log - high - middle
                for k, part in enumerate((high, middle, low)):
                    logs_held[n, 4 * k + head : 4 * k + head + 1, place] = part
        return carry

    lax.fori_loop(0, count * HALF_BLOCKS // 2, pair, 0)
    for n in range(count):
        outs[n][:rows, :] = told[n]
        outs[n][rows:, :] = logs_held[n].astype(jnp.bfloat16)


def lse_kernel(where_ref, *rest):
    pieces, keep_ref, give_ref, held = rest[:4], rest[4], rest[5], rest[6]
    core, chip = where_ref[0], where_ref[1]
    for r in range(CHIPS):
        parts = pieces[r][...].astype(jnp.float32)
        held[lax.rem(chip + r, CHIPS)] = parts[0:4] + parts[4:8] + parts[8:12]
    for j in range(2):
        keep_ref[4 * j : 4 * j + 4, :] = held[2 * core + j]
        give_ref[4 * j : 4 * j + 4, :] = held[2 * (1 - core) + j]


def finish_kernel(where_ref, *rest):
    pieces, w_ref, wp_ref, out_ref, held = rest[:4], rest[4], rest[5], rest[6], rest[7]
    core, chip = where_ref[0], where_ref[1]
    rows, width = held.shape[1:]
    for r in range(CHIPS):
        held[lax.rem(chip + r, CHIPS)] = pieces[r][:rows, :]
    projected = None
    for side, w in enumerate((w_ref, wp_ref)):
        owner = core if side == 0 else 1 - core
        for j in range(2):
            term = jnp.dot(
                held[2 * owner + j],
                w[j * width : (j + 1) * width, :],
                preferred_element_type=jnp.float32,
            )
            projected = term if projected is None else projected + term
    scale = lax.rsqrt(jnp.mean(projected * projected, axis=1, keepdims=True) + EPSILON)
    out_ref[...] = (projected * scale).astype(jnp.bfloat16)


SMEM = pl.BlockSpec(memory_space=pltpu.SMEM)
VMEM = pl.BlockSpec(memory_space=pltpu.VMEM)
ANY = pl.BlockSpec(memory_space=pl.ANY)


def grant(mib):
    return pltpu.CompilerParams(vmem_limit_bytes=mib * 2**20)


def attend(planes, slots, bias, queries, pieces):
    count = len(queries)
    rows, width = queries[0].shape[0] - EXTRA, queries[0].shape[1]
    total = 2 * planes * CHIPS * HALF_BLOCKS
    return pl.pallas_call(
        functools.partial(attend_kernel, count, planes),
        in_specs=[SMEM, SMEM] + [VMEM] * count + [ANY] * len(pieces),
        out_specs=[VMEM] * count,
        out_shape=[jax.ShapeDtypeStruct((rows + EXTRA, width), jnp.bfloat16)] * count,
        scratch_shapes=[
            pltpu.VMEM((total, BLK, LANES), jnp.bfloat16),
            pltpu.VMEM((count, rows, width), jnp.bfloat16),
            pltpu.VMEM((count, rows, width), jnp.bfloat16),
            pltpu.VMEM((count, EXTRA, rows), jnp.float32),
            pltpu.SemaphoreType.DMA((len(pieces),)),
        ],
        cost_estimate=pl.CostEstimate(
            flops=count * 32 * rows * width * (PICK + 1) * BLK,
            bytes_accessed=total * BLK * LANES * 2,
            transcendentals=0,
        ),
        compiler_params=grant(16),
        name="attend",
    )(slots, bias, *queries, *pieces)


def tied(value, *others):
    return lax.optimization_barrier((value,) + others)[0]


def shards(tokens, w_query, w_key, w_value, w_out, chosen):
    core = lax.axis_index("tp")
    index = lax.axis_index("kv")
    planes = lax.axis_size("kv") // CHIPS
    plane, chip = index // CHIPS, index % CHIPS
    here = jnp.stack([core, chip]).astype(jnp.int32)

    def partner(x):
        return lax.ppermute(x, "tp", [(0, 1), (1, 0)])

    def along_y(x, r):
        return lax.ppermute(
            x,
            "kv",
            [
                (z * CHIPS + y, z * CHIPS + (y + r) % CHIPS)
                for z in range(planes)
                for y in range(CHIPS)
            ],
        )

    def along_z(x, step):
        return lax.ppermute(
            x,
            "kv",
            [
                (z * CHIPS + y, (z + step) % planes * CHIPS + y)
                for z in range(planes)
                for y in range(CHIPS)
            ],
        )

    own = tokens[0]
    rows = own.shape[0]
    wk_peer, wv_peer = partner(w_key), partner(w_value)
    wq_peer = partner(tied(w_query, wk_peer, wv_peer))

    base = index * 2 * rows + core * rows
    cosine, sine = rotary_tables(base + jnp.arange(rows, dtype=jnp.int32))

    piece_shape = (HALF_BLOCKS, BLK, LANES)
    kv_out = pl.pallas_call(
        kv_kernel,
        in_specs=[SMEM] + [VMEM] * 7,
        out_specs=[VMEM] * CHIPS,
        out_shape=[jax.ShapeDtypeStruct(piece_shape, jnp.bfloat16)] * CHIPS,
        scratch_shapes=[pltpu.VMEM((CHIPS,) + piece_shape, jnp.bfloat16)],
        compiler_params=grant(8),
        name="project_kv",
    )(here, own, w_key, wk_peer, w_value, wv_peer, cosine, sine)
    kv_in = [kv_out[0]] + [along_y(kv_out[r], r) for r in range(1, CHIPS)]

    q_shape = (rows + EXTRA, 4 * HEAD_DIM)
    q_out = pl.pallas_call(
        q_kernel,
        in_specs=[SMEM] + [VMEM] * 6,
        out_specs=[VMEM] * CHIPS,
        out_shape=[jax.ShapeDtypeStruct(q_shape, jnp.bfloat16)] * CHIPS,
        scratch_shapes=[pltpu.VMEM((CHIPS, rows, 4 * HEAD_DIM), jnp.bfloat16)],
        compiler_params=grant(10),
        name="project_q",
    )(
        here,
        own,
        w_query,
        wq_peer,
        tied(cosine, kv_out[0]),
        sine,
        jnp.pad(chosen[0], ((0, 0), (0, LANES - PICK))),
    )
    start = jnp.stack(kv_in)

    chunks = {0: start}
    order = [0]
    up = down = start
    for n in range(1, planes // 2 + 1):
        up = along_z(up, 1)
        chunks[n] = up
        order.append(n)
        if n <= planes - 1 - planes // 2:
            down = along_z(down, -1)
            chunks[planes - n] = down
            order.append(planes - n)
    q_ready = [tied(q_out[r], chunks[1]) for r in range(CHIPS)]
    q_in = [q_ready[0]] + [along_y(q_ready[r], r) for r in range(1, CHIPS)]
    wo_peer = partner(tied(w_out, chunks[1]))

    flat = (CHIPS * HALF_BLOCKS, BLK, LANES)
    swapped = {}
    for at, d in enumerate(order):
        later = order[min(at + 2, len(order) - 1)]
        value = chunks[d] if later == d else tied(chunks[d], chunks[later])
        swapped[d] = partner(value)
    pieces = [chunks[d].reshape(flat) for d in range(planes)]
    pieces += [swapped[d].reshape(flat) for d in range(planes)]

    picks = jnp.stack([q[rows : rows + HALF_BLOCKS, :PICK] for q in q_in]).astype(jnp.int32)
    shift = jnp.arange(CHIPS, dtype=jnp.int32)
    source = (chip - shift) % CHIPS
    own_block = (
        plane * (8 * CHIPS)
        + source[:, None] * 8
        + core * HALF_BLOCKS
        + jnp.arange(HALF_BLOCKS, dtype=jnp.int32)[None, :]
    )
    blocks = jnp.concatenate([picks, own_block[:, :, None]], axis=2)
    bias = jnp.where(blocks >= 0, 0.0, NEGATIVE).astype(jnp.float32)
    blocks = jnp.maximum(blocks, 0)
    flag = (blocks // HALF_BLOCKS % 2) ^ core
    distance = (plane - blocks // (8 * CHIPS)) % planes
    turn = (chip - blocks // 8 % CHIPS) % CHIPS
    slots = ((flag * planes + distance) * CHIPS + turn) * HALF_BLOCKS + blocks % HALF_BLOCKS

    att = {}
    for shifts in ((2, 1, 3), (0,)):
        span = slice(1, None) if len(shifts) > 1 else slice(0, 1)
        names = sorted(shifts)
        done = attend(
            planes,
            slots[span].reshape(-1, PICK + 1),
            bias[span].reshape(-1, PICK + 1),
            [q_in[r] for r in names],
            pieces,
        )
        for n, r in enumerate(names):
            att[r] = along_y(done[n], -r) if r else done[n]

    tail = rows // EXTRA
    keep, give = pl.pallas_call(
        lse_kernel,
        grid=(1,),
        in_specs=[SMEM] + [pl.BlockSpec((EXTRA, rows), lambda i: (tail, 0))] * CHIPS,
        out_specs=[pl.BlockSpec((8, rows), lambda i: (0, 0))] * 2,
        out_shape=[jax.ShapeDtypeStruct((8, rows), jnp.float32)] * 2,
        scratch_shapes=[pltpu.VMEM((CHIPS, 4, rows), jnp.float32)],
        compiler_params=grant(4),
        name="sort_logsums",
    )(here, *[att[r] for r in range(CHIPS)])
    got = partner(give)
    normed = pl.pallas_call(
        finish_kernel,
        in_specs=[SMEM] + [VMEM] * (CHIPS + 2),
        out_specs=VMEM,
        out_shape=jax.ShapeDtypeStruct((rows, w_out.shape[1]), jnp.bfloat16),
        scratch_shapes=[pltpu.VMEM((CHIPS, rows, 4 * HEAD_DIM), jnp.bfloat16)],
        compiler_params=grant(10),
        name="finish",
    )(here, *[att[r] for r in range(CHIPS)], w_out, wo_peer)
    first = jnp.where(core == 0, keep, got)
    second = jnp.where(core == 0, got, keep)
    logsums = jnp.concatenate([first, second], axis=1).T
    return (normed[None], logsums[None])


def solution(mesh):
    placed = (
        P("dp", ("kv", "tp"), None),
        P(None, "tp"),
        P(None, "tp"),
        P(None, "tp"),
        P("tp", None),
        P("dp", "kv", None),
    )
    return jax.shard_map(
        shards,
        mesh=mesh,
        in_specs=placed,
        out_specs=(P("dp", ("kv", "tp"), None), P("dp", "kv", "tp")),
        check_vma=False,
    )
```
